32 devices in a mesh: rep: 2 (over x), fs: 8 (over z, y), tp: 2 (over core).
Axes of the slice: x: 2, y: 2, z: 4, core: 2. Of those that a mesh axis runs over, the one named last changes fastest.
Arguments:
- tokens: bfloat16 [8192, 2048], P(('rep', 'fs', 'tp')), may hold values from -6 to 6
- norm_gain: float32 [2048], replicated, may hold values from 0.1 to 1.9
- gate_weight: float32 [2048, 5120], P('fs', 'tp'), may hold values from -0.125 to 0.125
- gate_scale: float32 [5120], P('tp'), may hold values from 0.1 to 1.9
- up_weight: float32 [2048, 5120], P('fs', 'tp'), may hold values from -0.125 to 0.125
- up_scale: float32 [5120], P('tp'), may hold values from 0.1 to 1.9
- down_weight: float32 [5120, 2048], P('tp', 'fs'), may hold values from -0.078125 to 0.078125
- down_scale: float32 [2048], replicated, may hold values from 0.1 to 1.9
Outputs:
- mixed: bfloat16 [8192, 2048], P(('rep', 'fs', 'tp'))
The draws below stay inside these ranges and needn't reach their ends.
All inputs are finite; a program needn't handle non-finite values.
Results may differ from the reference program's by a relative error of at most 0.013.
Values may be sent and summed in bfloat16 or wider, within the bound.
A program may use at most 128 MiB of HBM per device.

```python
import jax
import jax.numpy as jnp
from jax import lax

D = 2048
FF = 5120
TOK_DEV = 256
TOKENS = 8192
N_TP = 2


def steps_of(key, shape, cuts, low, top_value):
    def one(position, blocks):
        steps = jax.random.uniform(jax.random.fold_in(jax.random.fold_in(key, 6), position), (blocks,), jnp.float32, low / len(cuts), top_value / len(cuts))
        return jnp.repeat(jnp.exp(steps), shape[position] // blocks).reshape((-1,) + (1,) * (len(shape) - position - 1))

    level = one(*cuts[0])
    for cut in cuts[1:]:
        level = level * one(*cut)
    return level


def bell_draw(key, extent, spread, limit, pieces=(), kind=jnp.bfloat16):
    drawn = spread * jax.random.normal(key, extent, jnp.float32)
    if pieces:
        drawn = drawn * steps_of(key, extent, pieces, -0.22, 0.18)
    return jnp.clip(drawn, -limit, limit).astype(kind)


def setup_inputs(seed: int = 0) -> dict:
    splits = jax.random.split(jax.random.key(seed), 9)
    return {
        "tokens": bell_draw(splits[0], (TOKENS, D), 1.0, 6.0, ((0, 32),)),
        "norm_gain": jnp.clip(1.0 + 0.18 * jax.random.normal(splits[1], (D,), jnp.float32), 0.1, 1.9),
        "gate_weight": bell_draw(splits[2], (D, FF), D ** -0.5, 0.125, ((0, 8), (1, 2)), jnp.float32),
        "gate_scale": jnp.clip(1.0 + 0.18 * jax.random.normal(splits[3], (FF,), jnp.float32), 0.1, 1.9),
        "up_weight": bell_draw(splits[4], (D, FF), D ** -0.5, 0.125, ((0, 8), (1, 2)), jnp.float32),
        "up_scale": jnp.clip(1.0 + 0.18 * jax.random.normal(splits[5], (FF,), jnp.float32), 0.1, 1.9),
        "down_weight": bell_draw(splits[6], (FF, D), FF ** -0.5, 0.078125, ((0, 2), (1, 8)), jnp.float32),
        "down_scale": jnp.clip(1.0 + 0.18 * jax.random.normal(splits[7], (D,), jnp.float32), 0.1, 1.9),
    }


EPS_VALUE = 1e-06

def normalize(token_rows, norm_gain):
    values = token_rows.astype(jnp.float32)
    inverse = lax.rsqrt(lax.optimization_barrier(jnp.mean(values * values, axis=-1, keepdims=True)) + EPS_VALUE)
    return (values * inverse * norm_gain).astype(jnp.bfloat16)

def reference(tokens, norm_gain, gate_weight, gate_scale, up_weight, up_scale, down_weight, down_scale):
    gate_bf = gate_weight.astype(jnp.bfloat16)
    up_bf = up_weight.astype(jnp.bfloat16)
    down_bf = down_weight.astype(jnp.bfloat16)
    width_tp = FF // N_TP
    down_blocks = down_bf.reshape(N_TP, width_tp, D)
    group_rows = TOK_DEV * N_TP

    def one_group(token_rows):
        normed = normalize(token_rows, norm_gain)
        gate_pre = jnp.dot(normed, gate_bf, preferred_element_type=jnp.float32) * gate_scale
        up_pre = jnp.dot(normed, up_bf, preferred_element_type=jnp.float32) * up_scale
        hidden = (jax.nn.silu(gate_pre) * up_pre).astype(jnp.bfloat16)
        total = jnp.zeros((group_rows, D), jnp.float32)
        for tp_block in range(N_TP):
            columns = hidden[:, tp_block * width_tp:(tp_block + 1) * width_tp]
            partial_value = (jnp.dot(columns, down_blocks[tp_block], preferred_element_type=jnp.float32) * down_scale).astype(jnp.bfloat16)
            partial_value = lax.optimization_barrier(partial_value)
            total = total + partial_value.astype(jnp.float32)
        return total.astype(jnp.bfloat16)
    grouped = tokens.reshape(TOKENS // group_rows, group_rows, D)
    return lax.map(one_group, grouped).reshape(TOKENS, D)
```

```python
import functools

import jax
import jax.numpy as jnp
from jax import lax
from jax.experimental import pallas as pl
from jax.experimental.pallas import tpu as pltpu
from jax.sharding import PartitionSpec as P

EPS_VALUE = 1e-06


def from_partner(shard, axis, distance):
    return lax.ppermute(shard, axis, [(i, i ^ 1 << distance) for i in range(lax.axis_size(axis))])


def normalize(token_rows, norm_gain):
    values = token_rows.astype(jnp.float32)
    inverse = lax.rsqrt(jnp.mean(values * values, axis=-1, keepdims=True) + EPS_VALUE)
    return (values * inverse * norm_gain).astype(jnp.bfloat16)


def body(tokens, norm_gain, gate_weight, gate_scale, up_weight, up_scale, down_weight, down_scale):
    normed = normalize(tokens, norm_gain)
    gate_bf = gate_weight.astype(jnp.bfloat16)
    up_bf = up_weight.astype(jnp.bfloat16)
    down_bf = down_weight.astype(jnp.bfloat16)
    rep_index = lax.axis_index("rep")
    half_cols = gate_bf.shape[1] // 2
    half_rows = down_bf.shape[0] // 2
    own_gate = lax.dynamic_slice_in_dim(gate_bf, rep_index * half_cols, half_cols, 1)
    own_up = lax.dynamic_slice_in_dim(up_bf, rep_index * half_cols, half_cols, 1)
    own_down = lax.dynamic_slice_in_dim(down_bf, rep_index * half_rows, half_rows, 0)
    own_parts = (
        lax.all_gather(own_gate, "fs", axis=0, tiled=True),
        lax.all_gather(own_up, "fs", axis=0, tiled=True),
        lax.all_gather(own_down, "fs", axis=1, tiled=True),
    )
    far_parts = from_partner((own_parts[0], own_parts[1], own_parts[2]), "rep", 0)
    is_first = rep_index == 0

    def joined(own_part, far_part, axis_dim):
        return jnp.where(
            is_first,
            jnp.concatenate([own_part, far_part], axis_dim),
            jnp.concatenate([far_part, own_part], axis_dim),
        )

    gate_full = joined(own_parts[0], far_parts[0], 1)
    up_full = joined(own_parts[1], far_parts[1], 1)
    down_full = joined(own_parts[2], far_parts[2], 0)
    slab_rows = lax.all_gather(normed, "tp", axis=0, tiled=True)
    gate_pre = jnp.dot(slab_rows, gate_full, preferred_element_type=jnp.float32) * gate_scale
    up_pre = jnp.dot(slab_rows, up_full, preferred_element_type=jnp.float32) * up_scale
    hidden = (jax.nn.silu(gate_pre) * up_pre).astype(jnp.bfloat16)
    partial_value = (
        jnp.dot(hidden, down_full, preferred_element_type=jnp.float32) * down_scale
    ).astype(jnp.bfloat16)
    partial_value = lax.optimization_barrier(partial_value)
    return lax.psum_scatter(
        partial_value.astype(jnp.float32).astype(jnp.bfloat16),
        "tp",
        scatter_dimension=0,
        tiled=True,
    )


MESH = pl.DeviceIdType.MESH
DOWN = 4


def ffn_kernel(
    sizes, tok_ref, gain_ref, gate_ref, gscale_ref, up_ref, uscale_ref, down_ref, dscale_ref, out_ref,
    raw_gu, raw_d, wgu, wd, tgu, td, scales, rows, acc, hid, staged, landed_x, summed, landed_z,
    load_sem, scale_send, scale_recv, pair_send, mid_send, main_recv, thru_recv, y_send, y_recv, c_send, c_recv,
    tok_send, tok_recv, px_send, px_recv, pz_send, pz_recv,
):
    n_tok = tok_ref.shape[0]
    half_tok = n_tok // 2
    units = tgu.shape[3]
    depth = tgu.shape[2]
    half = depth // 2
    cols = wd.shape[2]

    rep = lax.axis_index("rep")
    fs = lax.axis_index("fs")
    tp = lax.axis_index("tp")
    z = fs // 2
    y = fs % 2
    side_z = z // 2
    inner = (z + side_z) % 2
    outer = 1 - inner
    is_inner = inner == 1
    is_outer = inner == 0
    z_pair = 1 + 4 * side_z - z

    pair_dev = (rep, z_pair * 2 + y, tp)
    mid_dev = (rep, (3 - z) * 2 + y, tp)
    y_dev = (rep, z * 2 + 1 - y, tp)
    x_dev = (1 - rep, fs, tp)
    c_dev = (rep, fs, 1 - tp)

    def remote(src, dst, send, recv, device):
        return pltpu.make_async_remote_copy(
            src_ref=src, dst_ref=dst, send_sem=send, recv_sem=recv, device_id=device, device_id_type=MESH
        )

    def shard_z(turn, own=z, other=z_pair):
        if isinstance(turn, int):
            return (own, other, 2 - side_z, 3 - 3 * side_z)[turn]
        late = turn // 2
        odd = turn % 2
        early = (1 - odd) * own + odd * other
        return (1 - late) * early + late * ((1 - odd) * (2 - side_z) + odd * (3 - 3 * side_z))

    def main_at(shard, shard_y, part, core):
        lanes = pl.ds(pl.multiple_of(core * units, 128), units)
        if isinstance(part, int) and part == DOWN:
            return wd.at[shard * 2 + shard_y, lanes]
        start = pl.multiple_of(shard_y * depth + (part % 2) * half, half)
        return wgu.at[part // 2, shard, pl.ds(start, half), lanes]

    def thru_at(turn, part):
        if isinstance(part, int) and part == DOWN:
            return td.at[turn]
        start = pl.multiple_of((part % 2) * half, half)
        return tgu.at[part // 2, turn, pl.ds(start, half)]

    def pair_copy(kind, part):
        send = pair_send.at[kind, part]
        if kind == 0:
            return remote(thru_at(0, part), main_at(z, y, part, tp), send, main_recv.at[1, part], pair_dev)
        if kind == 1:
            return remote(main_at(z, y, part, tp), thru_at(1, part), send, thru_recv.at[1, part], pair_dev)
        return remote(
            thru_at(kind, part), main_at(shard_z(kind), y, part, tp), send, main_recv.at[kind, part], pair_dev
        )

    def mid_copy(kind, part):
        send = mid_send.at[kind, part]
        turn = 2 + kind // 2
        if kind % 2 == 0:
            ref = main_at(shard_z(kind // 2), y, part, tp)
            return remote(ref, ref, send, main_recv.at[turn, part], mid_dev)
        return remote(thru_at(kind // 2, part), thru_at(turn, part), send, thru_recv.at[turn, part], mid_dev)

    def main_in(turn, part):
        ref = main_at(shard_z(turn), y, part, tp)
        return remote(ref, ref, pair_send.at[0, part], main_recv.at[turn, part], pair_dev)

    def thru_in(turn, part):
        ref = thru_at(turn, part)
        return remote(ref, ref, pair_send.at[0, part], thru_recv.at[turn, part], pair_dev)

    def y_copy(turn, part):
        ref = main_at(shard_z(turn), y, part, tp)
        return remote(ref, ref, y_send.at[turn, part], y_recv.at[turn, part], y_dev)

    def y_in(turn, part):
        ref = main_at(shard_z(turn), 1 - y, part, tp)
        return remote(ref, ref, y_send.at[turn, part], y_recv.at[turn, part], y_dev)

    def c_copy(turn, side, part):
        ref = main_at(shard_z(turn), y + side - 2 * side * y, part, tp)
        return remote(ref, ref, c_send.at[turn, side, part], c_recv.at[turn, side, part], c_dev)

    def c_in(turn, side, part):
        ref = main_at(shard_z(turn), y + side - 2 * side * y, part, 1 - tp)
        return remote(ref, ref, c_send.at[turn, side, part], c_recv.at[turn, side, part], c_dev)

    def tok_pair(piece):
        part = pl.ds(piece * half_tok, half_tok)
        return remote(
            rows.at[0, part], rows.at[1, part], tok_send.at[piece], tok_recv.at[piece], pair_dev
        )

    def tok_x():
        return remote(
            rows.at[0, pl.ds(0, n_tok)], rows.at[0, pl.ds(n_tok, n_tok)], tok_send.at[2], tok_recv.at[2], x_dev
        )

    def tok_far(piece):
        return remote(
            rows.at[1, pl.ds(piece * half_tok, half_tok)], rows.at[1, pl.ds(n_tok + piece * half_tok, half_tok)],
            tok_send.at[3 + piece], tok_recv.at[3 + piece], x_dev,
        )

    def part_x(block, far):
        return remote(
            staged.at[block, far, 1], landed_x.at[block, far], px_send.at[block, far], px_recv.at[block, far], x_dev
        )

    def part_z(block):
        return remote(summed.at[block], landed_z.at[block], pz_send.at[block], pz_recv.at[block], pair_dev)

    def scale_copy():
        return remote(scales.at[tp], scales.at[tp], scale_send, scale_recv, c_dev)

    def scale_in():
        return remote(scales.at[1 - tp], scales.at[1 - tp], scale_send, scale_recv, c_dev)

    base = rep * 2 * units
    both = pl.ds(pl.multiple_of(base, 128), 2 * units)
    loads = []
    for part in range(4):
        source = gate_ref if part // 2 == 0 else up_ref
        span = pl.ds((part % 2) * half, half)
        loads.append(
            pltpu.make_async_copy(source.at[span, both], raw_gu.at[part // 2, span], load_sem.at[part])
        )
    loads.append(pltpu.make_async_copy(down_ref.at[both], raw_d, load_sem.at[DOWN]))
    for load in loads:
        load.start()
    barrier = pltpu.get_barrier_semaphore()
    for device in (pair_dev, y_dev, x_dev, c_dev):
        pl.semaphore_signal(barrier, inc=1, device_id=device, device_id_type=MESH)

    @pl.when(is_inner)
    def _():
        pl.semaphore_signal(barrier, inc=1, device_id=mid_dev, device_id_type=MESH)

    mine = pl.ds(pl.multiple_of(outer * units, 128), units)
    theirs = pl.ds(pl.multiple_of(inner * units, 128), units)
    lanes = pl.ds(pl.multiple_of(tp * units, 128), units)

    def round_part(part):
        loads[part].wait()
        span = slice((part % 2) * half, (part % 2 + 1) * half)
        start = pl.multiple_of(y * depth + (part % 2) * half, half)
        wgu[part // 2, z, pl.ds(start, half), lanes] = raw_gu[part // 2, span, mine].astype(jnp.bfloat16)
        tgu[part // 2, 0, span] = raw_gu[part // 2, span, theirs].astype(jnp.bfloat16)

    def send_part(part):
        y_copy(0, part).start()
        pair_copy(0, part).start()

        @pl.when(is_inner)
        def _():
            mid_copy(0, part).start()

        c_copy(0, 0, part).start()

    round_part(0)
    pl.semaphore_wait(barrier, 4 + inner)
    send_part(0)
    values = tok_ref[...].astype(jnp.float32)
    inverse = lax.rsqrt(jnp.mean(values * values, axis=-1, keepdims=True) + EPS_VALUE)
    rows[0, :n_tok] = (values * inverse * gain_ref[...]).astype(jnp.bfloat16)
    tok_x().start()
    for part in range(1, 4):
        round_part(part)
        send_part(part)
    for piece in range(2):
        tok_pair(piece).start()

    @pl.when(is_inner)
    def _():
        for part in range(4):
            mid_copy(1, part).start()

    @pl.when(is_outer)
    def _():
        for part in range(4):
            pair_copy(1, part).start()

    unit_cols = pl.ds(pl.multiple_of(base + outer * units, 128), units)
    scales[tp, 0:1] = gscale_ref[:, unit_cols]
    scales[tp, 1:2] = uscale_ref[:, unit_cols]
    scale_copy().start()
    loads[DOWN].wait()
    wd[fs, lanes] = raw_d[pl.ds(pl.multiple_of(outer * units, 128), units)].astype(jnp.bfloat16)
    td[0] = raw_d[pl.ds(pl.multiple_of(inner * units, 128), units)].astype(jnp.bfloat16)
    c_copy(0, 0, DOWN).start()

    @pl.when(is_outer)
    def _():
        pair_copy(0, DOWN).start()
        pair_copy(1, DOWN).start()

    def take_main(turn, part):
        main_in(turn, part).wait_recv()
        y_copy(turn, part).start()
        c_copy(turn, 0, part).start()

    def take_y(turn, part):
        y_in(turn, part).wait_recv()
        c_copy(turn, 1, part).start()

    def each(count, step):
        def go(index, carry):
            step(index)
            return carry

        lax.fori_loop(0, count, go, 0)

    def first(part):
        take_main(1, part)

        @pl.when(is_inner)
        def _():
            mid_copy(2, part).start()

        take_y(0, part)

    each(4, first)

    @pl.when(is_inner)
    def _():
        each(4, lambda part: take_main(2, part))

    def second(part):
        @pl.when(is_inner)
        def _():
            thru_in(2, part).wait_recv()
            pair_copy(2, part).start()

        take_y(1, part)

    each(4, second)
    for piece in range(2):
        tok_pair(piece).wait_recv()
        tok_far(piece).start()

    @pl.when(is_inner)
    def _():
        def third(part):
            take_main(3, part)
            take_y(2, part)

        each(4, third)

    @pl.when(is_outer)
    def _():
        each(4, lambda part: take_main(2, part))

    def c_wait(turn):
        def go(index):
            c_in(turn, index // 4, index % 4).wait_recv()

        each(8, go)

    tok_x().wait_recv()
    c_wait(0)
    c_wait(1)

    @pl.when(is_inner)
    def _():
        c_wait(2)

    def term(far, matrix, turn):
        shard = shard_z(turn)
        span = pl.ds(pl.multiple_of(shard * 2 * depth, 2 * depth), 2 * depth)
        return jnp.dot(rows[far, :, span], wgu[matrix, shard], preferred_element_type=jnp.float32)

    def add_third(far, matrix, low, high):
        def go(turn, carry):
            acc[matrix, far] += term(far, matrix, turn)
            return carry

        lax.fori_loop(low, high, go, 0)

    def fourth(part):
        far, matrix = part // 2, part % 2

        @pl.when(is_inner)
        def _():
            thru_in(1, part).wait_recv()
            mid_copy(3, part).start()

        @pl.when(part == 2)
        def _():
            for piece in range(2):
                tok_far(piece).wait_recv()

        acc[matrix, far] = term(far, matrix, 0)
        acc[matrix, far] += term(far, matrix, 1)
        add_third(far, matrix, 2, 2 + inner)

        @pl.when(is_inner)
        def _():
            thru_in(3, part).wait_recv()
            pair_copy(3, part).start()
            take_y(3, part)

        @pl.when(is_outer)
        def _():
            take_y(2, part)
            take_main(3, part)

    each(4, fourth)
    y_copy(0, DOWN).start()

    @pl.when(is_inner)
    def _():
        mid_copy(0, DOWN).start()
        mid_copy(1, DOWN).start()
        pair_copy(0, DOWN).start()

    @pl.when(is_outer)
    def _():
        c_wait(2)

    def fifth(part):
        add_third(part // 2, part % 2, 2 + inner, 3)

        @pl.when(is_outer)
        def _():
            take_y(3, part)

    each(4, fifth)
    scale_in().wait_recv()
    c_wait(3)

    def activate(far):
        gate_scale = jnp.concatenate([scales[0, 0:1], scales[1, 0:1]], axis=1)
        up_scale = jnp.concatenate([scales[0, 1:2], scales[1, 1:2]], axis=1)
        gate_pre = (acc[0, far] + term(far, 0, 3)) * gate_scale
        up_pre = (acc[1, far] + term(far, 1, 3)) * up_scale
        hid[far] = (jax.nn.silu(gate_pre) * up_pre).astype(jnp.bfloat16)

    each(2, activate)

    def block_of(turn, side, own=z, other=z_pair):
        return shard_z(turn, own, other) * 2 + y + side - 2 * side * y

    def produce(block):
        start = pl.multiple_of(block * cols, cols)
        scale = dscale_ref[:, pl.ds(start, cols)]

        def tile(far):
            product = jnp.dot(hid[far], wd[block], preferred_element_type=jnp.float32) * scale
            staged[block, far] = product.astype(jnp.bfloat16).reshape(2, n_tok, cols)
            part_x(block, far).start()

        each(2, tile)

    def down_step(step):
        @pl.when((step >= 1) & (step < 4))
        def _():
            take_main(step, DOWN)

            @pl.when(is_inner)
            def _():
                thru_in(step, DOWN).wait_recv()

                @pl.when(step == 1)
                def _():
                    mid_copy(2, DOWN).start()
                    mid_copy(3, DOWN).start()

                @pl.when(step == 2)
                def _():
                    pair_copy(2, DOWN).start()

                @pl.when(step == 3)
                def _():
                    pair_copy(3, DOWN).start()

        def sides(side):
            turn = step - side

            @pl.when((turn >= 0) & (turn < 4))
            def _():
                @pl.when(side == 1)
                def _():
                    take_y(turn, DOWN)

                c_in(turn, side, DOWN).wait_recv()
                produce(block_of(turn, side))

        each(2, sides)

    each(5, down_step)

    def in_order(visit):
        def step_of(step):
            def sides(side):
                @pl.when((step - side >= 0) & (step - side < 4))
                def _():
                    visit(step - side, side)

            each(2, sides)

        each(5, step_of)

    def reduce_block(turn, side):
        block = block_of(turn, side)
        for far in (1, 0):
            part_x(block, far).wait_recv()
        total = staged[block, 1, 0].astype(jnp.float32) + landed_x[block, 1].astype(jnp.float32)
        summed[block] = total.astype(jnp.bfloat16)
        part_z(block).start()

    in_order(reduce_block)

    def finish(turn, side):
        block = block_of(turn, side, z_pair, z)
        part_z(block).wait_recv()
        total = staged[block, 0, 0].astype(jnp.float32) + landed_x[block, 0].astype(jnp.float32)
        total = total + landed_z[block].astype(jnp.float32)
        out_ref[:, pl.ds(pl.multiple_of(block * cols, cols), cols)] = total.astype(out_ref.dtype)

    in_order(finish)

    def drain_part(part):
        pair_copy(0, part).wait_send()

        @pl.when(is_outer)
        def _():
            pair_copy(1, part).wait_send()

        @pl.when(is_inner)
        def _():
            pair_copy(2, part).wait_send()
            pair_copy(3, part).wait_send()
            for kind in range(4):
                mid_copy(kind, part).wait_send()

        def turns(turn):
            y_copy(turn, part).wait_send()
            c_copy(turn, 0, part).wait_send()
            c_copy(turn, 1, part).wait_send()

        each(4, turns)

    each(4, drain_part)
    drain_part(DOWN)
    for piece in range(2):
        tok_pair(piece).wait_send()
        tok_far(piece).wait_send()
    tok_x().wait_send()
    scale_copy().wait_send()

    def drain_block(block):
        part_x(block, 0).wait_send()
        part_x(block, 1).wait_send()
        part_z(block).wait_send()

    each(8, drain_block)


def kernel_body(sizes, tokens, norm_gain, gate_weight, gate_scale, up_weight, up_scale, down_weight, down_scale):
    n_fs = sizes[1]
    n_tok, width = tokens.shape
    depth = gate_weight.shape[0]
    units = gate_weight.shape[1] // (2 * sizes[0])
    cols = down_weight.shape[1]
    vmem = pl.BlockSpec(memory_space=pltpu.VMEM)
    anywhere = pl.BlockSpec(memory_space=pl.ANY)
    bf, wide = jnp.bfloat16, jnp.float32
    dma = pltpu.SemaphoreType.DMA
    return pl.pallas_call(
        functools.partial(ffn_kernel, sizes),
        out_shape=jax.ShapeDtypeStruct((n_tok, width), bf),
        in_specs=[vmem, vmem, anywhere, vmem, anywhere, vmem, anywhere, vmem],
        out_specs=vmem,
        scratch_shapes=[
            pltpu.VMEM((2, depth, 2 * units), wide),
            pltpu.VMEM((2 * units, cols), wide),
            pltpu.VMEM((2, n_fs // 2, 2 * depth, 2 * units), bf),
            pltpu.VMEM((n_fs, 2 * units, cols), bf),
            pltpu.VMEM((2, 4, depth, units), bf),
            pltpu.VMEM((4, units, cols), bf),
            pltpu.VMEM((2, 2, units), wide),
            pltpu.VMEM((2, 2 * n_tok, width), bf),
            pltpu.VMEM((2, 2, 2 * n_tok, 2 * units), wide),
            pltpu.VMEM((2, 2 * n_tok, 2 * units), bf),
            pltpu.VMEM((n_fs, 2, 2, n_tok, cols), bf),
            pltpu.VMEM((n_fs, 2, n_tok, cols), bf),
            pltpu.VMEM((n_fs, n_tok, cols), bf),
            pltpu.VMEM((n_fs, n_tok, cols), bf),
            dma((5,)), dma, dma,
            dma((4, 5)), dma((4, 5)), dma((4, 5)), dma((4, 5)), dma((4, 5)), dma((4, 5)),
            dma((4, 2, 5)), dma((4, 2, 5)),
            dma((5,)), dma((5,)),
            dma((n_fs, 2)), dma((n_fs, 2)), dma((n_fs,)), dma((n_fs,)),
        ],
        compiler_params=pltpu.CompilerParams(
            collective_id=0, has_side_effects=True, vmem_limit_bytes=62 * 1024 * 1024
        ),
    )(
        tokens, norm_gain[None, :], gate_weight, gate_scale[None, :], up_weight, up_scale[None, :],
        down_weight, down_scale[None, :],
    )


def fits_kernel(mesh, tokens, gate_weight, down_weight):
    n_rep, n_fs, n_tp = (mesh.shape[name] for name in ("rep", "fs", "tp"))
    units = gate_weight.shape[1] // (n_tp * n_rep * 2)
    aligned = units % 128 == 0 and down_weight.shape[1] // n_fs % 128 == 0
    return aligned and n_rep == 2 and n_fs == 8 and n_tp == 2


def solution(mesh):
    sizes = tuple(mesh.shape[name] for name in ("rep", "fs", "tp"))

    def run(tokens, norm_gain, gate_weight, gate_scale, up_weight, up_scale, down_weight, down_scale):
        chosen = body
        if fits_kernel(mesh, tokens, gate_weight, down_weight):
            chosen = functools.partial(kernel_body, sizes)
        return jax.shard_map(
            chosen,
            mesh=mesh,
            in_specs=(
                P(("rep", "fs", "tp"), None),
                P(),
                P("fs", "tp"),
                P("tp"),
                P("fs", "tp"),
                P("tp"),
                P("tp", "fs"),
                P(),
            ),
            out_specs=P(("rep", "fs", "tp"), None),
            check_vma=False,
        )(tokens, norm_gain, gate_weight, gate_scale, up_weight, up_scale, down_weight, down_scale)

    return run
```

```python
import functools

import jax
import jax.numpy as jnp
from jax import lax
from jax.experimental import pallas as pl
from jax.experimental.pallas import tpu as pltpu
from jax.sharding import PartitionSpec as P

EPS_VALUE = 1e-06


def from_partner(shard, axis, distance):
    return lax.ppermute(shard, axis, [(i, i ^ 1 << distance) for i in range(lax.axis_size(axis))])


def normalize(token_rows, norm_gain):
    values = token_rows.astype(jnp.float32)
    inverse = lax.rsqrt(jnp.mean(values * values, axis=-1, keepdims=True) + EPS_VALUE)
    return (values * inverse * norm_gain).astype(jnp.bfloat16)


def body(tokens, norm_gain, gate_weight, gate_scale, up_weight, up_scale, down_weight, down_scale):
    normed = normalize(tokens, norm_gain)
    gate_bf = gate_weight.astype(jnp.bfloat16)
    up_bf = up_weight.astype(jnp.bfloat16)
    down_bf = down_weight.astype(jnp.bfloat16)
    rep_index = lax.axis_index("rep")
    half_cols = gate_bf.shape[1] // 2
    half_rows = down_bf.shape[0] // 2
    own_gate = lax.dynamic_slice_in_dim(gate_bf, rep_index * half_cols, half_cols, 1)
    own_up = lax.dynamic_slice_in_dim(up_bf, rep_index * half_cols, half_cols, 1)
    own_down = lax.dynamic_slice_in_dim(down_bf, rep_index * half_rows, half_rows, 0)
    own_parts = (
        lax.all_gather(own_gate, "fs", axis=0, tiled=True),
        lax.all_gather(own_up, "fs", axis=0, tiled=True),
        lax.all_gather(own_down, "fs", axis=1, tiled=True),
    )
    far_parts = from_partner((own_parts[0], own_parts[1], own_parts[2]), "rep", 0)
    is_first = rep_index == 0

    def joined(own_part, far_part, axis_dim):
        return jnp.where(
            is_first,
            jnp.concatenate([own_part, far_part], axis_dim),
            jnp.concatenate([far_part, own_part], axis_dim),
        )

    gate_full = joined(own_parts[0], far_parts[0], 1)
    up_full = joined(own_parts[1], far_parts[1], 1)
    down_full = joined(own_parts[2], far_parts[2], 0)
    slab_rows = lax.all_gather(normed, "tp", axis=0, tiled=True)
    gate_pre = jnp.dot(slab_rows, gate_full, preferred_element_type=jnp.float32) * gate_scale
    up_pre = jnp.dot(slab_rows, up_full, preferred_element_type=jnp.float32) * up_scale
    hidden = (jax.nn.silu(gate_pre) * up_pre).astype(jnp.bfloat16)
    partial_value = (
        jnp.dot(hidden, down_full, preferred_element_type=jnp.float32) * down_scale
    ).astype(jnp.bfloat16)
    partial_value = lax.optimization_barrier(partial_value)
    return lax.psum_scatter(
        partial_value.astype(jnp.float32).astype(jnp.bfloat16),
        "tp",
        scatter_dimension=0,
        tiled=True,
    )


MESH = pl.DeviceIdType.MESH
DOWN = 4
PIECES = 4


def each(count, step):
    def go(index, carry):
        step(index)
        return carry

    lax.fori_loop(0, count, go, 0)


def ffn_kernel(
    tok_ref, gain_ref, gate_ref, gscale_ref, up_ref, uscale_ref, down_ref, dscale_ref, out_ref,
    tok, gain, gscale, uscale, dscale, raw_gu, raw_d, wgu, wd, tgu, td, scales, rows, acc, hid,
    staged, landed_x, summed, landed_z, landed_f, result,
    load_sem, out_sem, scale_send, scale_recv, pair_send, mid_send, main_recv, thru_recv, y_send, y_recv, c_send,
    c_recv, tok_send, tok_recv, px_send, px_recv, pz_send, pz_recv, pf_send, pf_recv,
):
    n_tok = tok.shape[0]
    piece_tok = n_tok // PIECES
    units = tgu.shape[3]
    depth = tgu.shape[2]
    half = depth // 2
    cols = wd.shape[2]

    rep = lax.axis_index("rep")
    fs = lax.axis_index("fs")
    tp = lax.axis_index("tp")
    z = fs // 2
    y = fs % 2
    side_z = z // 2
    inner = (z + side_z) % 2
    outer = 1 - inner
    is_inner = inner == 1
    is_outer = inner == 0
    z_pair = 1 + 4 * side_z - z

    pair_dev = (rep, z_pair * 2 + y, tp)
    mid_dev = (rep, (3 - z) * 2 + y, tp)
    y_dev = (rep, z * 2 + 1 - y, tp)
    x_dev = (1 - rep, fs, tp)
    c_dev = (rep, fs, 1 - tp)

    barrier = pltpu.get_barrier_semaphore()
    for device in (pair_dev, y_dev, x_dev, c_dev):
        pl.semaphore_signal(barrier, inc=1, device_id=device, device_id_type=MESH)

    @pl.when(is_inner)
    def _():
        pl.semaphore_signal(barrier, inc=1, device_id=mid_dev, device_id_type=MESH)

    def remote(src, dst, send, recv, device):
        return pltpu.make_async_remote_copy(
            src_ref=src, dst_ref=dst, send_sem=send, recv_sem=recv, device_id=device, device_id_type=MESH
        )

    def shard_z(turn):
        if isinstance(turn, int):
            return (z, z_pair, 2 - side_z, 3 - 3 * side_z)[turn]
        late = turn // 2
        odd = turn % 2
        early = (1 - odd) * z + odd * z_pair
        return (1 - late) * early + late * ((1 - odd) * (2 - side_z) + odd * (3 - 3 * side_z))

    def main_at(shard, shard_y, part, core):
        lanes = pl.ds(pl.multiple_of(core * units, 128), units)
        if isinstance(part, int) and part == DOWN:
            return wd.at[shard * 2 + shard_y, lanes]
        start = pl.multiple_of(shard_y * depth + (part % 2) * half, half)
        return wgu.at[part // 2, shard, pl.ds(start, half), lanes]

    def thru_at(turn, part):
        if isinstance(part, int) and part == DOWN:
            return td.at[turn]
        start = pl.multiple_of((part % 2) * half, half)
        return tgu.at[part // 2, turn, pl.ds(start, half)]

    def pair_copy(kind, part):
        send = pair_send.at[kind, part]
        if kind == 0:
            return remote(thru_at(0, part), main_at(z, y, part, tp), send, main_recv.at[1, part], pair_dev)
        if kind == 1:
            return remote(main_at(z, y, part, tp), thru_at(1, part), send, thru_recv.at[1, part], pair_dev)
        return remote(
            thru_at(kind, part), main_at(shard_z(kind), y, part, tp), send, main_recv.at[kind, part], pair_dev
        )

    def mid_copy(kind, part):
        send = mid_send.at[kind, part]
        turn = 2 + kind // 2
        if kind % 2 == 0:
            ref = main_at(shard_z(kind // 2), y, part, tp)
            return remote(ref, ref, send, main_recv.at[turn, part], mid_dev)
        return remote(thru_at(kind // 2, part), thru_at(turn, part), send, thru_recv.at[turn, part], mid_dev)

    def main_in(turn, part):
        ref = main_at(shard_z(turn), y, part, tp)
        return remote(ref, ref, pair_send.at[0, part], main_recv.at[turn, part], pair_dev)

    def thru_in(turn, part):
        ref = thru_at(turn, part)
        return remote(ref, ref, pair_send.at[0, part], thru_recv.at[turn, part], pair_dev)

    def y_copy(turn, part):
        ref = main_at(shard_z(turn), y, part, tp)
        return remote(ref, ref, y_send.at[turn, part], y_recv.at[turn, part], y_dev)

    def y_in(turn, part):
        ref = main_at(shard_z(turn), 1 - y, part, tp)
        return remote(ref, ref, y_send.at[turn, part], y_recv.at[turn, part], y_dev)

    def c_copy(turn, side, part):
        ref = main_at(shard_z(turn), y + side - 2 * side * y, part, tp)
        return remote(ref, ref, c_send.at[turn, side, part], c_recv.at[turn, side, part], c_dev)

    def c_in(turn, side, part):
        ref = main_at(shard_z(turn), y + side - 2 * side * y, part, 1 - tp)
        return remote(ref, ref, c_send.at[turn, side, part], c_recv.at[turn, side, part], c_dev)

    def tok_pair(piece):
        part = pl.ds(piece * piece_tok, piece_tok)
        return remote(
            rows.at[0, part], rows.at[1, part], tok_send.at[piece], tok_recv.at[piece], pair_dev
        )

    def tok_far(piece):
        return remote(
            rows.at[1, pl.ds(piece * piece_tok, piece_tok)],
            rows.at[1, pl.ds(n_tok + piece * piece_tok, piece_tok)],
            tok_send.at[PIECES + piece], tok_recv.at[PIECES + piece], x_dev,
        )

    def tok_x():
        return remote(
            rows.at[0, pl.ds(0, n_tok)], rows.at[0, pl.ds(n_tok, n_tok)],
            tok_send.at[2 * PIECES], tok_recv.at[2 * PIECES], x_dev,
        )

    def part_x(block, far):
        return remote(
            staged.at[block, far, 1], landed_x.at[block, far], px_send.at[block, far], px_recv.at[block, far], x_dev
        )

    def part_z(block):
        return remote(summed.at[block], landed_z.at[block], pz_send.at[block], pz_recv.at[block], pair_dev)

    def early_z(block):
        return remote(staged.at[block, 1, 0], landed_z.at[block], pz_send.at[block], pz_recv.at[block], pair_dev)

    def place_of(turn):
        late = turn // 2
        return (1 - late) * (shard_z(turn) - 2 * side_z) + 2 * late

    def early_far(block, place):
        return remote(
            staged.at[block, 1, 1], landed_f.at[place], pf_send.at[place], pf_recv.at[place], pair_dev
        )

    def scale_copy():
        return remote(scales.at[tp], scales.at[tp], scale_send, scale_recv, c_dev)

    def scale_in():
        return remote(scales.at[1 - tp], scales.at[1 - tp], scale_send, scale_recv, c_dev)

    base = rep * 2 * units
    both = pl.ds(pl.multiple_of(base, 128), 2 * units)
    loads = []
    for part in range(4):
        source = gate_ref if part // 2 == 0 else up_ref
        span = pl.ds((part % 2) * half, half)
        loads.append((source.at[span, both], raw_gu.at[part // 2, span]))
    loads.append((down_ref.at[both], raw_d))
    loads += [(tok_ref, tok), (gain_ref, gain), (gscale_ref, gscale), (uscale_ref, uscale), (dscale_ref, dscale)]
    loads = [pltpu.make_async_copy(*pair, load_sem.at[index]) for index, pair in enumerate(loads)]
    for index in (0, 5, 6, 1, 2, 3, 4, 7, 8, 9):
        loads[index].start()

    mine = pl.ds(pl.multiple_of(outer * units, 128), units)
    theirs = pl.ds(pl.multiple_of(inner * units, 128), units)
    lanes = pl.ds(pl.multiple_of(tp * units, 128), units)

    def round_part(part):
        loads[part].wait()
        span = slice((part % 2) * half, (part % 2 + 1) * half)
        start = pl.multiple_of(y * depth + (part % 2) * half, half)
        wgu[part // 2, z, pl.ds(start, half), lanes] = raw_gu[part // 2, span, mine].astype(jnp.bfloat16)
        tgu[part // 2, 0, span] = raw_gu[part // 2, span, theirs].astype(jnp.bfloat16)

    def send_part(part):
        pair_copy(0, part).start()
        y_copy(0, part).start()

        @pl.when(is_inner)
        def _():
            mid_copy(0, part).start()

        c_copy(0, 0, part).start()

    round_part(0)
    pl.semaphore_wait(barrier, 4 + inner)
    send_part(0)
    loads[5].wait()
    loads[6].wait()
    values = tok[...].astype(jnp.float32)
    inverse = lax.rsqrt(jnp.mean(values * values, axis=-1, keepdims=True) + EPS_VALUE)
    rows[0, :n_tok] = (values * inverse * gain[...]).astype(jnp.bfloat16)
    tok_x().start()
    for part in range(1, 4):
        round_part(part)
        send_part(part)
    for piece in range(PIECES):
        tok_pair(piece).start()

    @pl.when(is_inner)
    def _():
        for part in range(4):
            mid_copy(1, part).start()

    @pl.when(is_outer)
    def _():
        for part in range(4):
            pair_copy(1, part).start()

    for index in (7, 8, 9):
        loads[index].wait()
    first_row = (base + outer * units) // 128
    for index in range(units // 128):
        span = slice(index * 128, (index + 1) * 128)
        scales[tp, 0:1, span] = gscale[pl.ds(first_row + index, 1), :]
        scales[tp, 1:2, span] = uscale[pl.ds(first_row + index, 1), :]
    scale_copy().start()
    loads[DOWN].wait()
    wd[fs, lanes] = raw_d[mine].astype(jnp.bfloat16)
    td[0] = raw_d[theirs].astype(jnp.bfloat16)
    c_copy(0, 0, DOWN).start()

    @pl.when(is_outer)
    def _():
        pair_copy(0, DOWN).start()
        pair_copy(1, DOWN).start()

    def take_main(turn, part):
        main_in(turn, part).wait_recv()
        y_copy(turn, part).start()
        c_copy(turn, 0, part).start()

    def take_y(turn, part):
        y_in(turn, part).wait_recv()
        c_copy(turn, 1, part).start()

    def take_rows(piece):
        tok_pair(piece).wait_recv()
        tok_far(piece).start()

    def c_wait(turn):
        each(8, lambda index: c_in(turn, index // 4, index % 4).wait_recv())

    def term(far, matrix, turn):
        shard = shard_z(turn)
        span = pl.ds(pl.multiple_of(shard * 2 * depth, 2 * depth), 2 * depth)
        return jnp.dot(rows[far, :, span], wgu[matrix, shard], preferred_element_type=jnp.float32)

    def add_early(part):
        far, matrix = part // 2, part % 2

        @pl.when(part == 2)
        def _():
            for piece in range(PIECES):
                tok_far(piece).wait_recv()

        acc[matrix, far] = term(far, matrix, 0)
        acc[matrix, far] += term(far, matrix, 1)

    def add_late(part):
        acc[part % 2, part // 2] += term(part // 2, part % 2, 2)

    def first(part):
        take_main(1, part)

        @pl.when(is_inner)
        def _():
            mid_copy(2, part).start()

        take_y(0, part)

    each(4, first)

    @pl.when(is_inner)
    def _():
        each(4, lambda part: take_main(2, part))

    @pl.when(is_outer)
    def _():
        y_copy(0, DOWN).start()

    def second(part):
        @pl.when(is_inner)
        def _():
            thru_in(2, part).wait_recv()
            pair_copy(2, part).start()

        take_y(1, part)

        @pl.when((part == 1) | (part == 2))
        def _():
            take_rows(part - 1)

    each(4, second)
    take_rows(2)

    def pass_outward(part):
        thru_in(1, part).wait_recv()
        mid_copy(3, part).start()

    @pl.when(is_inner)
    def _():
        def third(part):
            take_main(3, part)
            take_y(2, part)

            @pl.when(part == 1)
            def _():
                take_rows(3)

            @pl.when(part == 2)
            def _():
                pass_outward(0)

        each(4, third)
        y_copy(0, DOWN).start()

    @pl.when(is_outer)
    def _():
        take_rows(3)

    tok_x().wait_recv()
    c_wait(0)
    c_wait(1)

    @pl.when(is_inner)
    def _():
        c_wait(2)

        def fourth(part):
            @pl.when(part < 3)
            def _():
                pass_outward(part + 1)

            @pl.when(part == 2)
            def _():
                mid_copy(1, DOWN).start()
                mid_copy(0, DOWN).start()

            add_early(part)
            add_late(part)
            thru_in(3, part).wait_recv()
            pair_copy(3, part).start()
            take_y(3, part)

        each(4, fourth)
        pair_copy(0, DOWN).start()

    @pl.when(is_outer)
    def _():
        def fourth(part):
            take_main(2, part)

            @pl.when(part > 0)
            def _():
                take_y(2, part - 1)

            add_early(part)

        each(4, fourth)

        def fifth(part):
            take_main(3, part)

            @pl.when(part == 0)
            def _():
                take_y(2, 3)
                c_wait(2)

            @pl.when(part > 0)
            def _():
                take_y(3, part - 1)

            add_late(part)

        each(4, fifth)
        take_y(3, 3)
        take_y(0, DOWN)
        c_in(0, 1, DOWN).wait_recv()

    def block_of(turn, side):
        return shard_z(turn) * 2 + y + side - 2 * side * y

    def z_first(turn, side):
        return ((side == 1) & (turn < 2)) | ((side == 0) & (turn == 2))

    def send_off(turn, side, far, near_x):
        block = block_of(turn, side)
        ahead = z_first(turn, side)
        crossing = far + inner == 1

        @pl.when((near_x == 1) & (jnp.logical_not(ahead) | jnp.logical_not(crossing)))
        def _():
            part_x(block, far).start()

        @pl.when(ahead & crossing & is_outer)
        def _():
            @pl.when(near_x == 1)
            def _():
                early_far(block, place_of(turn)).start()

            @pl.when(near_x == 0)
            def _():
                early_z(block).start()

    def scale_of(block):
        return dscale[:, pl.ds(pl.multiple_of(block * cols, cols), cols)]

    scale_in().wait_recv()
    c_wait(3)
    c_in(0, 0, DOWN).wait_recv()

    def activate(index):
        swap = (index + 1) // 2 % 2
        far = inner + swap - 2 * inner * swap
        near_x = 1 - index // 2
        span = pl.ds(pl.multiple_of(near_x * n_tok, n_tok), n_tok)
        shard = shard_z(3)
        depths = pl.ds(pl.multiple_of(shard * 2 * depth, 2 * depth), 2 * depth)
        pre = []
        for matrix in range(2):
            last = jnp.dot(rows[far, span, depths], wgu[matrix, shard], preferred_element_type=jnp.float32)
            scale = jnp.concatenate(
                [scales[0, matrix:matrix + 1], scales[1, matrix:matrix + 1]], axis=1
            )
            pre.append((acc[matrix, far, span] + last) * scale)
        hid[far, span] = (jax.nn.silu(pre[0]) * pre[1]).astype(jnp.bfloat16)

        def one(side, carry):
            block = block_of(0, side)
            product = jnp.dot(hid[far, span], wd[block], preferred_element_type=jnp.float32) * scale_of(block)
            staged[block, far, near_x] = product.astype(jnp.bfloat16)
            send_off(0, side, far, near_x)
            return carry

        lax.fori_loop(0, 1 + outer, one, 0)

    each(4, activate)

    def produce(turn, side):
        block = block_of(turn, side)

        def tile(index):
            far = 1 - index
            product = jnp.dot(hid[far], wd[block], preferred_element_type=jnp.float32) * scale_of(block)
            staged[block, far] = product.astype(jnp.bfloat16).reshape(2, n_tok, cols)
            for near_x in (1, 0):
                send_off(turn, side, far, near_x)

        each(2, tile)

    def fold(turn, side):
        block = block_of(turn, side)

        @pl.when(is_inner | jnp.logical_not(z_first(turn, side)))
        def _():
            part_x(block, 1).wait_recv()
            total = staged[block, 1, 0].astype(jnp.float32) + landed_x[block, 1].astype(jnp.float32)
            summed[block] = total.astype(jnp.bfloat16)
            part_z(block).start()

    def late_x(turn, side):
        block = block_of(turn, side)
        place = place_of(turn)
        early_far(block, place).wait_recv()
        total = staged[block, 0, 1].astype(jnp.float32) + landed_f[place].astype(jnp.float32)
        staged[block, 0, 1] = total.astype(jnp.bfloat16)
        part_x(block, 0).start()

    def down_step(index):
        step = index + 1
        swap = inner * (step // 3) * (1 - step // 4)

        @pl.when(is_inner & (step == 4))
        def _():
            late_x(0, 1)

        def sides(order):
            side = order + swap - 2 * order * swap
            turn = step - side

            @pl.when((turn < 4) & ((side == 0) | (turn > 0) | is_inner))
            def _():
                @pl.when(side == 0)
                def _():
                    take_main(turn, DOWN)

                @pl.when(side == 1)
                def _():
                    take_y(turn, DOWN)

                c_in(turn, side, DOWN).wait_recv()
                produce(turn, side)

        each(2, sides)

        @pl.when(is_inner)
        def _():
            @pl.when(step == 1)
            def _():
                thru_in(2, DOWN).wait_recv()
                pair_copy(2, DOWN).start()
                thru_in(1, DOWN).wait_recv()
                mid_copy(3, DOWN).start()
                mid_copy(2, DOWN).start()

            @pl.when(step == 2)
            def _():
                thru_in(3, DOWN).wait_recv()
                pair_copy(3, DOWN).start()

            @pl.when(step == 3)
            def _():
                late_x(1, 1)

        def folds(side):
            @pl.when(step - 1 - side >= 0)
            def _():
                fold(step - 1 - side, side)

        each(2, folds)

    each(4, down_step)
    fold(3, 1)

    @pl.when(is_inner)
    def _():
        late_x(2, 0)

    def out_copy(block):
        span = pl.ds(pl.multiple_of(block * cols, cols), cols)
        return pltpu.make_async_copy(result.at[:, span], out_ref.at[:, span], out_sem.at[block])

    def finish(index):
        block = block_of(outer * (index // 2) + inner * (3 - index // 2), index % 2)
        part_x(block, 0).wait_recv()
        part_z(block).wait_recv()
        total = staged[block, 0, 0].astype(jnp.float32) + landed_x[block, 0].astype(jnp.float32)
        total = total + landed_z[block].astype(jnp.float32)
        result[:, pl.ds(pl.multiple_of(block * cols, cols), cols)] = total.astype(result.dtype)
        out_copy(block).start()

    each(8, finish)

    def drain_part(part):
        pair_copy(0, part).wait_send()

        @pl.when(is_outer)
        def _():
            pair_copy(1, part).wait_send()

        @pl.when(is_inner)
        def _():
            pair_copy(2, part).wait_send()
            pair_copy(3, part).wait_send()
            for kind in range(4):
                mid_copy(kind, part).wait_send()

        def turns(turn):
            y_copy(turn, part).wait_send()
            c_copy(turn, 0, part).wait_send()
            c_copy(turn, 1, part).wait_send()

        each(4, turns)

    each(4, drain_part)
    drain_part(DOWN)

    def drain_rows(piece):
        tok_pair(piece).wait_send()
        tok_far(piece).wait_send()

    each(PIECES, drain_rows)
    tok_x().wait_send()
    scale_copy().wait_send()

    def drain_block(turn):
        def sides(side):
            block = block_of(turn, side)
            part_x(block, 0).wait_send()
            part_z(block).wait_send()
            ahead = z_first(turn, side)

            @pl.when(is_inner | jnp.logical_not(ahead))
            def _():
                part_x(block, 1).wait_send()

            @pl.when(is_outer & ahead)
            def _():
                early_far(block, place_of(turn)).wait_send()

            out_copy(block).wait()

        each(2, sides)

    each(4, drain_block)


def kernel_body(tokens, norm_gain, gate_weight, gate_scale, up_weight, up_scale, down_weight, down_scale, sizes):
    n_fs = sizes[1]
    n_tok, width = tokens.shape
    depth = gate_weight.shape[0]
    all_units = gate_weight.shape[1]
    units = all_units // (2 * sizes[0])
    cols = down_weight.shape[1]
    anywhere = pl.BlockSpec(memory_space=pl.ANY)
    bf, wide = jnp.bfloat16, jnp.float32
    dma = pltpu.SemaphoreType.DMA
    turns, parts = 4, 5
    return pl.pallas_call(
        ffn_kernel,
        out_shape=jax.ShapeDtypeStruct((n_tok, width), bf),
        in_specs=[anywhere] * 8,
        out_specs=anywhere,
        scratch_shapes=[
            pltpu.VMEM((n_tok, width), bf),
            pltpu.VMEM((1, width), wide),
            pltpu.VMEM((all_units // 128, 128), wide),
            pltpu.VMEM((all_units // 128, 128), wide),
            pltpu.VMEM((1, width), wide),
            pltpu.VMEM((2, depth, 2 * units), wide),
            pltpu.VMEM((2 * units, cols), wide),
            pltpu.VMEM((2, n_fs // 2, 2 * depth, 2 * units), bf),
            pltpu.VMEM((n_fs, 2 * units, cols), bf),
            pltpu.VMEM((2, turns, depth, units), bf),
            pltpu.VMEM((turns, units, cols), bf),
            pltpu.VMEM((2, 2, units), wide),
            pltpu.VMEM((2, 2 * n_tok, width), bf),
            pltpu.VMEM((2, 2, 2 * n_tok, 2 * units), wide),
            pltpu.VMEM((2, 2 * n_tok, 2 * units), bf),
            pltpu.VMEM((n_fs, 2, 2, n_tok, cols), bf),
            pltpu.VMEM((n_fs, 2, n_tok, cols), bf),
            pltpu.VMEM((n_fs, n_tok, cols), bf),
            pltpu.VMEM((n_fs, n_tok, cols), bf),
            pltpu.VMEM((3, n_tok, cols), bf),
            pltpu.VMEM((n_tok, width), bf),
            dma((10,)), dma((n_fs,)), dma, dma,
            dma((turns, parts)), dma((turns, parts)), dma((turns, parts)), dma((turns, parts)),
            dma((turns, parts)), dma((turns, parts)), dma((turns, 2, parts)), dma((turns, 2, parts)),
            dma((2 * PIECES + 1,)), dma((2 * PIECES + 1,)),
            dma((n_fs, 2)), dma((n_fs, 2)), dma((n_fs,)), dma((n_fs,)), dma((3,)), dma((3,)),
        ],
        compiler_params=pltpu.CompilerParams(
            collective_id=0, has_side_effects=True, vmem_limit_bytes=62 * 1024 * 1024
        ),
    )(
        tokens, norm_gain[None, :], gate_weight, gate_scale.reshape(-1, 128), up_weight, up_scale.reshape(-1, 128),
        down_weight, down_scale[None, :],
    )


def fits_kernel(mesh, tokens, gate_weight, down_weight):
    n_rep, n_fs, n_tp = (mesh.shape[name] for name in ("rep", "fs", "tp"))
    units = gate_weight.shape[1] // (n_tp * n_rep * 2)
    aligned = units % 128 == 0 and down_weight.shape[1] // n_fs % 128 == 0
    return aligned and n_rep == 2 and n_fs == 8 and n_tp == 2


def solution(mesh):
    sizes = tuple(mesh.shape[name] for name in ("rep", "fs", "tp"))

    def run(tokens, norm_gain, gate_weight, gate_scale, up_weight, up_scale, down_weight, down_scale):
        chosen = body
        if fits_kernel(mesh, tokens, gate_weight, down_weight):
            chosen = functools.partial(kernel_body, sizes=sizes)
        return jax.shard_map(
            chosen,
            mesh=mesh,
            in_specs=(
                P(("rep", "fs", "tp"), None),
                P(),
                P("fs", "tp"),
                P("tp"),
                P("fs", "tp"),
                P("tp"),
                P("tp", "fs"),
                P(),
            ),
            out_specs=P(("rep", "fs", "tp"), None),
            check_vma=False,
        )(tokens, norm_gain, gate_weight, gate_scale, up_weight, up_scale, down_weight, down_scale)

    return run
```

```python
import functools

import jax
import jax.numpy as jnp
from jax import lax
from jax.experimental import pallas as pl
from jax.experimental.pallas import tpu as pltpu
from jax.sharding import PartitionSpec as P

EPS_VALUE = 1e-06


def from_partner(shard, axis, distance):
    return lax.ppermute(shard, axis, [(i, i ^ 1 << distance) for i in range(lax.axis_size(axis))])


def normalize(token_rows, norm_gain):
    values = token_rows.astype(jnp.float32)
    inverse = lax.rsqrt(jnp.mean(values * values, axis=-1, keepdims=True) + EPS_VALUE)
    return (values * inverse * norm_gain).astype(jnp.bfloat16)


def body(tokens, norm_gain, gate_weight, gate_scale, up_weight, up_scale, down_weight, down_scale):
    normed = normalize(tokens, norm_gain)
    gate_bf = gate_weight.astype(jnp.bfloat16)
    up_bf = up_weight.astype(jnp.bfloat16)
    down_bf = down_weight.astype(jnp.bfloat16)
    rep_index = lax.axis_index("rep")
    half_cols = gate_bf.shape[1] // 2
    half_rows = down_bf.shape[0] // 2
    own_gate = lax.dynamic_slice_in_dim(gate_bf, rep_index * half_cols, half_cols, 1)
    own_up = lax.dynamic_slice_in_dim(up_bf, rep_index * half_cols, half_cols, 1)
    own_down = lax.dynamic_slice_in_dim(down_bf, rep_index * half_rows, half_rows, 0)
    own_parts = (
        lax.all_gather(own_gate, "fs", axis=0, tiled=True),
        lax.all_gather(own_up, "fs", axis=0, tiled=True),
        lax.all_gather(own_down, "fs", axis=1, tiled=True),
    )
    far_parts = from_partner((own_parts[0], own_parts[1], own_parts[2]), "rep", 0)
    is_first = rep_index == 0

    def joined(own_part, far_part, axis_dim):
        return jnp.where(
            is_first,
            jnp.concatenate([own_part, far_part], axis_dim),
            jnp.concatenate([far_part, own_part], axis_dim),
        )

    gate_full = joined(own_parts[0], far_parts[0], 1)
    up_full = joined(own_parts[1], far_parts[1], 1)
    down_full = joined(own_parts[2], far_parts[2], 0)
    slab_rows = lax.all_gather(normed, "tp", axis=0, tiled=True)
    gate_pre = jnp.dot(slab_rows, gate_full, preferred_element_type=jnp.float32) * gate_scale
    up_pre = jnp.dot(slab_rows, up_full, preferred_element_type=jnp.float32) * up_scale
    hidden = (jax.nn.silu(gate_pre) * up_pre).astype(jnp.bfloat16)
    partial_value = (
        jnp.dot(hidden, down_full, preferred_element_type=jnp.float32) * down_scale
    ).astype(jnp.bfloat16)
    partial_value = lax.optimization_barrier(partial_value)
    return lax.psum_scatter(
        partial_value.astype(jnp.float32).astype(jnp.bfloat16),
        "tp",
        scatter_dimension=0,
        tiled=True,
    )


MESH = pl.DeviceIdType.MESH
CUTS = 4
DOWN = 2 * CUTS
PIECES = 4


def each(count, step):
    def go(index, carry):
        step(index)
        return carry

    lax.fori_loop(0, count, go, 0)


def ffn_kernel(
    tok_ref, gain_ref, gate_ref, gscale_ref, up_ref, uscale_ref, down_ref, dscale_ref, out_ref,
    tok, gain, gscale, uscale, dscale, raw_gu, raw_d, wgu, wd, tgu, td, scales, rows, acc, hid,
    staged, landed_x, summed, landed_z, landed_f, result,
    load_sem, out_sem, scale_send, scale_recv, pair_send, mid_send, main_recv, thru_recv, y_send, y_recv, c_send,
    c_recv, tok_send, tok_recv, px_send, px_recv, pz_send, pz_recv, pf_send, pf_recv,
):
    n_tok = tok.shape[0]
    piece_tok = n_tok // PIECES
    units = tgu.shape[3]
    depth = tgu.shape[2]
    fine = depth // CUTS
    cols = wd.shape[2]

    rep = lax.axis_index("rep")
    fs = lax.axis_index("fs")
    tp = lax.axis_index("tp")
    z = fs // 2
    y = fs % 2
    side_z = z // 2
    inner = (z + side_z) % 2
    outer = 1 - inner
    is_inner = inner == 1
    is_outer = inner == 0
    z_pair = 1 + 4 * side_z - z

    pair_dev = (rep, z_pair * 2 + y, tp)
    mid_dev = (rep, (3 - z) * 2 + y, tp)
    y_dev = (rep, z * 2 + 1 - y, tp)
    x_dev = (1 - rep, fs, tp)
    c_dev = (rep, fs, 1 - tp)

    barrier = pltpu.get_barrier_semaphore()
    for device in (pair_dev, y_dev, x_dev, c_dev):
        pl.semaphore_signal(barrier, inc=1, device_id=device, device_id_type=MESH)

    @pl.when(is_inner)
    def _():
        pl.semaphore_signal(barrier, inc=1, device_id=mid_dev, device_id_type=MESH)

    def remote(src, dst, send, recv, device):
        return pltpu.make_async_remote_copy(
            src_ref=src, dst_ref=dst, send_sem=send, recv_sem=recv, device_id=device, device_id_type=MESH
        )

    def shard_z(turn):
        if isinstance(turn, int):
            return (z, z_pair, 2 - side_z, 3 - 3 * side_z)[turn]
        late = turn // 2
        odd = turn % 2
        early = (1 - odd) * z + odd * z_pair
        return (1 - late) * early + late * ((1 - odd) * (2 - side_z) + odd * (3 - 3 * side_z))

    def main_at(shard, shard_y, part, core):
        lanes = pl.ds(pl.multiple_of(core * units, 128), units)
        if isinstance(part, int) and part == DOWN:
            return wd.at[shard * 2 + shard_y, lanes]
        start = pl.multiple_of(shard_y * depth + (part % CUTS) * fine, fine)
        return wgu.at[part // CUTS, shard, pl.ds(start, fine), lanes]

    def thru_at(turn, part):
        if isinstance(part, int) and part == DOWN:
            return td.at[turn]
        start = pl.multiple_of((part % CUTS) * fine, fine)
        return tgu.at[part // CUTS, turn, pl.ds(start, fine)]

    def kind_of(part):
        return 1 if isinstance(part, int) and part == DOWN else 0

    def pair_copy(kind, part):
        send = pair_send.at[kind_of(part)]
        if kind == 0:
            return remote(thru_at(0, part), main_at(z, y, part, tp), send, main_recv.at[0, part], pair_dev)
        if kind == 1:
            return remote(main_at(z, y, part, tp), thru_at(1, part), send, thru_recv.at[0, part], pair_dev)
        return remote(
            thru_at(kind, part), main_at(shard_z(kind), y, part, tp), send, main_recv.at[kind - 1, part], pair_dev
        )

    def mid_copy(kind, part):
        send = mid_send.at[kind_of(part)]
        turn = 2 + kind // 2
        if kind % 2 == 0:
            ref = main_at(shard_z(kind // 2), y, part, tp)
            return remote(ref, ref, send, main_recv.at[turn - 1, part], mid_dev)
        return remote(thru_at(kind // 2, part), thru_at(turn, part), send, thru_recv.at[turn - 1, part], mid_dev)

    def main_in(turn, part):
        ref = main_at(shard_z(turn), y, part, tp)
        return remote(ref, ref, pair_send.at[0], main_recv.at[turn - 1, part], pair_dev)

    def thru_in(turn, part):
        ref = thru_at(turn, part)
        return remote(ref, ref, pair_send.at[0], thru_recv.at[turn - 1, part], pair_dev)

    def y_copy(turn, part):
        ref = main_at(shard_z(turn), y, part, tp)
        return remote(ref, ref, y_send.at[kind_of(part)], y_recv.at[turn, part], y_dev)

    def y_in(turn, part):
        ref = main_at(shard_z(turn), 1 - y, part, tp)
        return remote(ref, ref, y_send.at[kind_of(part)], y_recv.at[turn, part], y_dev)

    def c_copy(turn, side, part):
        ref = main_at(shard_z(turn), y + side - 2 * side * y, part, tp)
        return remote(ref, ref, c_send.at[kind_of(part)], c_recv.at[turn, side, kind_of(part)], c_dev)

    def c_in(turn, side, part):
        shard_y = y + side - 2 * side * y
        if part == DOWN:
            ref = main_at(shard_z(turn), shard_y, DOWN, 1 - tp)
        else:
            spare = pl.ds(pl.multiple_of((1 - tp) * units, 128), units)
            start = pl.multiple_of(shard_y * depth, depth)
            ref = wgu.at[:, shard_z(turn), pl.ds(start, depth), spare]
        return remote(ref, ref, c_send.at[kind_of(part)], c_recv.at[turn, side, kind_of(part)], c_dev)

    def tok_pair(piece):
        part = pl.ds(piece * piece_tok, piece_tok)
        return remote(
            rows.at[0, part], rows.at[1, part], tok_send.at[0], tok_recv.at[piece], pair_dev
        )

    def tok_far(piece):
        return remote(
            rows.at[1, pl.ds(piece * piece_tok, piece_tok)],
            rows.at[1, pl.ds(n_tok + piece * piece_tok, piece_tok)],
            tok_send.at[1], tok_recv.at[PIECES + piece], x_dev,
        )

    def tok_x():
        return remote(
            rows.at[0, pl.ds(0, n_tok)], rows.at[0, pl.ds(n_tok, n_tok)],
            tok_send.at[2], tok_recv.at[2 * PIECES], x_dev,
        )

    def part_x(block, far):
        return remote(
            staged.at[block, far, 1], landed_x.at[block, far], px_send, px_recv.at[block, far], x_dev
        )

    def part_z(block):
        return remote(summed.at[block], landed_z.at[block], pz_send, pz_recv.at[block], pair_dev)

    def early_z(block):
        return remote(staged.at[block, 1, 0], landed_z.at[block], pz_send, pz_recv.at[block], pair_dev)

    def place_of(turn, side):
        return side * (shard_z(turn) - 2 * side_z) + (1 - side) * (2 + turn // 2)

    def early_far(block, place):
        return remote(
            staged.at[block, 1, 1], landed_f.at[place], pf_send, pf_recv.at[place], pair_dev
        )

    def scale_copy():
        return remote(scales.at[tp], scales.at[tp], scale_send, scale_recv, c_dev)

    def scale_in():
        return remote(scales.at[1 - tp], scales.at[1 - tp], scale_send, scale_recv, c_dev)

    base = rep * 2 * units
    both = pl.ds(pl.multiple_of(base, 128), 2 * units)
    loads = []
    for part in range(DOWN):
        source = gate_ref if part // CUTS == 0 else up_ref
        span = pl.ds((part % CUTS) * fine, fine)
        loads.append((source.at[span, both], raw_gu.at[part // CUTS, span]))
    loads.append((down_ref.at[both], raw_d))
    loads += [(tok_ref, tok), (gain_ref, gain), (gscale_ref, gscale), (uscale_ref, uscale), (dscale_ref, dscale)]
    loads = [pltpu.make_async_copy(*pair, load_sem.at[index]) for index, pair in enumerate(loads)]
    for index in (0, 1, DOWN + 1, DOWN + 2, *range(2, DOWN + 1), DOWN + 3, DOWN + 4, DOWN + 5):
        loads[index].start()

    mine = pl.ds(pl.multiple_of(outer * units, 128), units)
    theirs = pl.ds(pl.multiple_of(inner * units, 128), units)
    lanes = pl.ds(pl.multiple_of(tp * units, 128), units)

    def round_part(part):
        loads[part].wait()
        span = slice((part % CUTS) * fine, (part % CUTS + 1) * fine)
        start = pl.multiple_of(y * depth + (part % CUTS) * fine, fine)
        wgu[part // CUTS, z, pl.ds(start, fine), lanes] = raw_gu[part // CUTS, span, mine].astype(jnp.bfloat16)
        tgu[part // CUTS, 0, span] = raw_gu[part // CUTS, span, theirs].astype(jnp.bfloat16)

    def send_part(part):
        pair_copy(0, part).start()
        y_copy(0, part).start()

        @pl.when(is_inner)
        def _():
            mid_copy(0, part).start()

        c_copy(0, 0, part).start()

    round_part(0)
    pl.semaphore_wait(barrier, 4 + inner)
    send_part(0)
    round_part(1)
    send_part(1)
    loads[DOWN + 1].wait()
    loads[DOWN + 2].wait()
    values = tok[...].astype(jnp.float32)
    inverse = lax.rsqrt(jnp.mean(values * values, axis=-1, keepdims=True) + EPS_VALUE)
    rows[0, :n_tok] = (values * inverse * gain[...]).astype(jnp.bfloat16)
    tok_x().start()
    for part in range(2, DOWN):
        round_part(part)
        send_part(part)
    for piece in range(PIECES):
        tok_pair(piece).start()

    @pl.when(is_inner)
    def _():
        each(DOWN, lambda part: mid_copy(1, part).start())

    @pl.when(is_outer)
    def _():
        each(DOWN, lambda part: pair_copy(1, part).start())

    for index in (DOWN + 3, DOWN + 4, DOWN + 5):
        loads[index].wait()
    first_row = (base + outer * units) // 128
    for index in range(units // 128):
        span = slice(index * 128, (index + 1) * 128)
        scales[tp, 0:1, span] = gscale[pl.ds(first_row + index, 1), :]
        scales[tp, 1:2, span] = uscale[pl.ds(first_row + index, 1), :]
    scale_copy().start()
    loads[DOWN].wait()
    wd[fs, lanes] = raw_d[mine].astype(jnp.bfloat16)
    td[0] = raw_d[theirs].astype(jnp.bfloat16)
    c_copy(0, 0, DOWN).start()

    @pl.when(is_outer)
    def _():
        pair_copy(0, DOWN).start()
        pair_copy(1, DOWN).start()

    def take_main(turn, part):
        main_in(turn, part).wait_recv()
        y_copy(turn, part).start()
        c_copy(turn, 0, part).start()

    def take_y(turn, part):
        y_in(turn, part).wait_recv()
        c_copy(turn, 1, part).start()

    def take_rows(piece):
        tok_pair(piece).wait_recv()
        tok_far(piece).start()

    def c_wait(turn):
        for side in range(2):
            c_in(turn, side, 0).wait_recv()

    def term(far, matrix, turn):
        shard = shard_z(turn)
        span = pl.ds(pl.multiple_of(shard * 2 * depth, 2 * depth), 2 * depth)
        return jnp.dot(rows[far, :, span], wgu[matrix, shard], preferred_element_type=jnp.float32)

    def add_early(part):
        far, matrix = part // 2, part % 2

        @pl.when(part == 2)
        def _():
            for piece in range(PIECES):
                tok_far(piece).wait_recv()

        acc[matrix, far] = term(far, matrix, 0)
        acc[matrix, far] += term(far, matrix, 1)

    def add_late(part):
        acc[part % 2, part // 2] += term(part // 2, part % 2, 2)

    def half_term(far, matrix, span, side):
        shard = shard_z(3)
        shard_y = y + side - 2 * side * y
        start = pl.multiple_of((shard * 2 + shard_y) * depth, depth)
        inside = pl.multiple_of(shard_y * depth, depth)
        return jnp.dot(
            rows[far, span, pl.ds(start, depth)], wgu[matrix, shard, pl.ds(inside, depth)],
            preferred_element_type=jnp.float32,
        )

    def add_last(part):
        acc[part % 2, part // 2] += half_term(part // 2, part % 2, pl.ds(0, 2 * n_tok), 0)

    def first(part):
        take_main(1, part)

        @pl.when(is_inner)
        def _():
            mid_copy(2, part).start()

        take_y(0, part)

    each(DOWN, first)

    @pl.when(is_inner)
    def _():
        each(DOWN, lambda part: take_main(2, part))

    @pl.when(is_outer)
    def _():
        y_copy(0, DOWN).start()

    def second(part):
        @pl.when(is_inner)
        def _():
            thru_in(2, part).wait_recv()
            pair_copy(2, part).start()

        take_y(1, part)

        @pl.when((part == 3) | (part == 5))
        def _():
            take_rows((part - 3) // 2)

    each(DOWN, second)
    take_rows(2)

    def pass_outward(part):
        thru_in(1, part).wait_recv()
        mid_copy(3, part).start()

    @pl.when(is_inner)
    def _():
        def third(part):
            take_main(3, part)
            take_y(2, part)

            @pl.when(part == 3)
            def _():
                take_rows(3)

            @pl.when(part > 5)
            def _():
                pass_outward(part - 6)

        each(DOWN, third)
        y_copy(0, DOWN).start()

    @pl.when(is_outer)
    def _():
        take_rows(3)

    tok_x().wait_recv()
    c_wait(0)
    c_wait(1)

    @pl.when(is_inner)
    def _():
        c_wait(2)
        c_in(3, 0, 0).wait_recv()

        def fourth(chunk):
            @pl.when(chunk < 3)
            def _():
                for ahead in (2, 3):
                    pass_outward(2 * chunk + ahead)

            @pl.when(chunk == 2)
            def _():
                mid_copy(1, DOWN).start()
                mid_copy(0, DOWN).start()

            add_early(chunk)
            add_late(chunk)
            for part in (2 * chunk, 2 * chunk + 1):
                thru_in(3, part).wait_recv()
                pair_copy(3, part).start()
                take_y(3, part)
            add_last(chunk)

        each(4, fourth)
        pair_copy(0, DOWN).start()

    @pl.when(is_outer)
    def _():
        def fourth(chunk):
            for part in (2 * chunk, 2 * chunk + 1):
                take_main(2, part)

                @pl.when(chunk > 0)
                def _():
                    take_y(2, part - 2)

            add_early(chunk)

        each(4, fourth)

        def fifth(chunk):
            for part in (2 * chunk, 2 * chunk + 1):
                take_main(3, part)

                @pl.when(chunk == 0)
                def _():
                    take_y(2, part + 6)

                @pl.when(chunk > 0)
                def _():
                    take_y(3, part - 2)

            @pl.when(chunk == 0)
            def _():
                c_wait(2)

            add_late(chunk)

        each(4, fifth)
        c_in(3, 0, 0).wait_recv()
        take_y(3, 6)
        each(2, add_last)
        take_y(3, 7)
        each(2, lambda chunk: add_last(chunk + 2))
        take_y(0, DOWN)
        c_in(0, 1, DOWN).wait_recv()

    def block_of(turn, side):
        return shard_z(turn) * 2 + y + side - 2 * side * y

    def z_first(turn, side):
        return ((turn < 2) & ((side == 1) | (turn + inner == 1))) | ((turn == 2) & (side == 0))

    def send_off(turn, side, far, near_x):
        block = block_of(turn, side)
        ahead = z_first(turn, side)
        crossing = far + inner == 1

        held = is_outer & (turn == 2) & (side == 1) & (far == 0)

        @pl.when((near_x == 1) & jnp.logical_not((ahead & crossing) | held))
        def _():
            part_x(block, far).start()

        @pl.when(ahead & crossing & is_outer)
        def _():
            @pl.when(near_x == 1)
            def _():
                early_far(block, place_of(turn, side)).start()

            @pl.when(near_x == 0)
            def _():
                early_z(block).start()

    def scale_of(block):
        return dscale[:, pl.ds(pl.multiple_of(block * cols, cols), cols)]

    scale_in().wait_recv()
    c_in(3, 1, 0).wait_recv()
    c_in(0, 0, DOWN).wait_recv()

    def activate(index):
        swap = (index + 1) // 2 % 2
        far = inner + swap - 2 * inner * swap
        near_x = 1 - index // 2
        span = pl.ds(pl.multiple_of(near_x * n_tok, n_tok), n_tok)
        pre = []

        @pl.when(index == 1 + inner)
        def _():
            take_main(1, DOWN)

        for matrix in range(2):
            last = half_term(far, matrix, span, 1)
            scale = jnp.concatenate(
                [scales[0, matrix:matrix + 1], scales[1, matrix:matrix + 1]], axis=1
            )
            pre.append((acc[matrix, far, span] + last) * scale)
        hid[far, span] = (jax.nn.silu(pre[0]) * pre[1]).astype(jnp.bfloat16)

        def one(side, carry):
            block = block_of(0, side)
            product = jnp.dot(hid[far, span], wd[block], preferred_element_type=jnp.float32) * scale_of(block)
            staged[block, far, near_x] = product.astype(jnp.bfloat16)
            send_off(0, side, far, near_x)
            return carry

        lax.fori_loop(0, 1 + outer, one, 0)

    each(4, activate)

    def produce(turn, side):
        block = block_of(turn, side)

        def tile(index):
            far = 1 - index
            product = jnp.dot(hid[far], wd[block], preferred_element_type=jnp.float32) * scale_of(block)
            staged[block, far] = product.astype(jnp.bfloat16).reshape(2, n_tok, cols)
            for near_x in (1, 0):
                send_off(turn, side, far, near_x)

        each(2, tile)

    def fold(turn, side):
        block = block_of(turn, side)

        @pl.when(is_inner | jnp.logical_not(z_first(turn, side)))
        def _():
            part_x(block, 1).wait_recv()
            total = staged[block, 1, 0].astype(jnp.float32) + landed_x[block, 1].astype(jnp.float32)
            summed[block] = total.astype(jnp.bfloat16)
            part_z(block).start()

    def late_x(turn, side):
        block = block_of(turn, side)
        place = place_of(turn, side)
        early_far(block, place).wait_recv()
        total = staged[block, 0, 1].astype(jnp.float32) + landed_f[place].astype(jnp.float32)
        staged[block, 0, 1] = total.astype(jnp.bfloat16)
        part_x(block, 0).start()

    def down_step(index):
        step = index + 1
        swap = inner * (step // 3) * (1 - step // 4)

        @pl.when(is_inner & (step == 2))
        def _():
            take_main(2, DOWN)

        @pl.when(is_inner | (step > 1))
        def _():
            take_y(step - 1, DOWN)

        def sides(order):
            side = order + swap - 2 * order * swap
            turn = step - side

            @pl.when((turn < 4) & ((side == 0) | (turn > 0) | is_inner))
            def _():
                @pl.when(is_inner & (side == 0) & (turn == 3))
                def _():
                    take_main(3, DOWN)

                c_in(turn, side, DOWN).wait_recv()
                produce(turn, side)

        each(2, sides)

        @pl.when(is_inner)
        def _():
            @pl.when(step == 1)
            def _():
                thru_in(2, DOWN).wait_recv()
                pair_copy(2, DOWN).start()
                thru_in(1, DOWN).wait_recv()
                mid_copy(3, DOWN).start()
                mid_copy(2, DOWN).start()

            @pl.when(step == 2)
            def _():
                thru_in(3, DOWN).wait_recv()
                pair_copy(3, DOWN).start()

            @pl.when(step == 3)
            def _():
                late_x(1, 1)

            @pl.when(step == 4)
            def _():
                late_x(0, 0)
                late_x(0, 1)

        @pl.when(is_outer & (step < 3))
        def _():
            take_main(step + 1, DOWN)

        @pl.when(is_outer & (step == 4))
        def _():
            part_x(block_of(2, 1), 0).start()

        def folds(side):
            later = outer * (1 - side) * (1 - (step - 1) // 2)

            @pl.when((step - 1 - side >= 0) & (is_inner | (side == 1) | (step > 1)))
            def _():
                fold(step - 1 - side - later, side)

        each(2, folds)

    each(4, down_step)


    @pl.when(is_inner)
    def _():
        late_x(2, 0)

    fold(3, 1)

    def out_copy(block):
        span = pl.ds(pl.multiple_of(block * cols, cols), cols)
        return pltpu.make_async_copy(result.at[:, span], out_ref.at[:, span], out_sem)

    def finish(index):
        block = block_of(outer * (index // 2) + inner * (3 - index // 2), index % 2)
        part_x(block, 0).wait_recv()
        part_z(block).wait_recv()
        total = staged[block, 0, 0].astype(jnp.float32) + landed_x[block, 0].astype(jnp.float32)
        total = total + landed_z[block].astype(jnp.float32)
        result[:, pl.ds(pl.multiple_of(block * cols, cols), cols)] = total.astype(result.dtype)
        out_copy(block).start()

    each(8, finish)

    def sent(src, send):
        remote(src, src, send, pf_recv.at[0], c_dev).wait_send()

    near = pl.ds(0, units)

    def drain(turns, pair_turns):
        for count, send in ((pair_turns, pair_send), (turns, mid_send)):
            if count:
                sent(wgu.at[:, pl.ds(0, count), pl.ds(0, depth), near], send.at[0])
                sent(wd.at[pl.ds(0, count), near], send.at[1])

    @pl.when(is_inner)
    def _():
        drain(4, 3)
        sent(staged.at[pl.ds(0, 4)], px_send)

    @pl.when(is_outer)
    def _():
        drain(0, 2)
        sent(staged.at[pl.ds(0, 3)], px_send)
        sent(landed_f, pf_send)

    sent(wgu.at[:, :, pl.ds(0, depth), near], y_send.at[0])
    sent(wd.at[pl.ds(0, 4), near], y_send.at[1])
    sent(wgu.at[:, :, :, near], c_send.at[0])
    sent(wd.at[:, near], c_send.at[1])
    for index in range(3):
        sent(rows.at[0, pl.ds(0, n_tok)], tok_send.at[index])
    scale_copy().wait_send()
    sent(landed_z, pz_send)
    pltpu.make_async_copy(result, out_ref, out_sem).wait()


def kernel_body(tokens, norm_gain, gate_weight, gate_scale, up_weight, up_scale, down_weight, down_scale, sizes):
    n_fs = sizes[1]
    n_tok, width = tokens.shape
    depth = gate_weight.shape[0]
    all_units = gate_weight.shape[1]
    units = all_units // (2 * sizes[0])
    cols = down_weight.shape[1]
    anywhere = pl.BlockSpec(memory_space=pl.ANY)
    bf, wide = jnp.bfloat16, jnp.float32
    dma = pltpu.SemaphoreType.DMA
    turns, parts = 4, DOWN + 1
    return pl.pallas_call(
        ffn_kernel,
        out_shape=jax.ShapeDtypeStruct((n_tok, width), bf),
        in_specs=[anywhere] * 8,
        out_specs=anywhere,
        scratch_shapes=[
            pltpu.VMEM((n_tok, width), bf),
            pltpu.VMEM((1, width), wide),
            pltpu.VMEM((all_units // 128, 128), wide),
            pltpu.VMEM((all_units // 128, 128), wide),
            pltpu.VMEM((1, width), wide),
            pltpu.VMEM((2, depth, 2 * units), wide),
            pltpu.VMEM((2 * units, cols), wide),
            pltpu.VMEM((2, n_fs // 2, 2 * depth, 2 * units), bf),
            pltpu.VMEM((n_fs, 2 * units, cols), bf),
            pltpu.VMEM((2, turns, depth, units), bf),
            pltpu.VMEM((turns, units, cols), bf),
            pltpu.VMEM((2, 2, units), wide),
            pltpu.VMEM((2, 2 * n_tok, width), bf),
            pltpu.VMEM((2, 2, 2 * n_tok, 2 * units), wide),
            pltpu.VMEM((2, 2 * n_tok, 2 * units), bf),
            pltpu.VMEM((n_fs, 2, 2, n_tok, cols), bf),
            pltpu.VMEM((n_fs, 2, n_tok, cols), bf),
            pltpu.VMEM((n_fs, n_tok, cols), bf),
            pltpu.VMEM((n_fs, n_tok, cols), bf),
            pltpu.VMEM((4, n_tok, cols), bf),
            pltpu.VMEM((n_tok, width), bf),
            dma((DOWN + 6,)), dma, dma, dma,
            dma((2,)), dma((2,)), dma((turns - 1, parts)), dma((turns - 1, parts)),
            dma((2,)), dma((turns, parts)), dma((2,)), dma((turns, 2, 2)),
            dma((3,)), dma((2 * PIECES + 1,)),
            dma, dma((n_fs, 2)), dma, dma((n_fs,)), dma, dma((4,)),
        ],
        compiler_params=pltpu.CompilerParams(
            collective_id=0, has_side_effects=True, vmem_limit_bytes=62 * 1024 * 1024
        ),
    )(
        tokens, norm_gain[None, :], gate_weight, gate_scale.reshape(-1, 128), up_weight, up_scale.reshape(-1, 128),
        down_weight, down_scale[None, :],
    )


def fits_kernel(mesh, tokens, gate_weight, down_weight):
    n_rep, n_fs, n_tp = (mesh.shape[name] for name in ("rep", "fs", "tp"))
    units = gate_weight.shape[1] // (n_tp * n_rep * 2)
    aligned = units % 128 == 0 and down_weight.shape[1] // n_fs % 128 == 0
    aligned = aligned and gate_weight.shape[0] // n_fs % (32 * CUTS) == 0
    return aligned and n_rep == 2 and n_fs == 8 and n_tp == 2


def solution(mesh):
    sizes = tuple(mesh.shape[name] for name in ("rep", "fs", "tp"))

    def run(tokens, norm_gain, gate_weight, gate_scale, up_weight, up_scale, down_weight, down_scale):
        chosen = body
        if fits_kernel(mesh, tokens, gate_weight, down_weight):
            chosen = functools.partial(kernel_body, sizes=sizes)
        return jax.shard_map(
            chosen,
            mesh=mesh,
            in_specs=(
                P(("rep", "fs", "tp"), None),
                P(),
                P("fs", "tp"),
                P("tp"),
                P("fs", "tp"),
                P("tp"),
                P("tp", "fs"),
                P(),
            ),
            out_specs=P(("rep", "fs", "tp"), None),
            check_vma=False,
        )(tokens, norm_gain, gate_weight, gate_scale, up_weight, up_scale, down_weight, down_scale)

    return run
```

```python
import functools

import jax
import jax.numpy as jnp
from jax import lax
from jax.experimental import pallas as pl
from jax.experimental.pallas import tpu as pltpu
from jax.sharding import PartitionSpec as P

EPS_VALUE = 1e-06


def from_partner(shard, axis, distance):
    return lax.ppermute(shard, axis, [(i, i ^ 1 << distance) for i in range(lax.axis_size(axis))])


def normalize(token_rows, norm_gain):
    values = token_rows.astype(jnp.float32)
    inverse = lax.rsqrt(jnp.mean(values * values, axis=-1, keepdims=True) + EPS_VALUE)
    return (values * inverse * norm_gain).astype(jnp.bfloat16)


def body(tokens, norm_gain, gate_weight, gate_scale, up_weight, up_scale, down_weight, down_scale):
    normed = normalize(tokens, norm_gain)
    gate_bf = gate_weight.astype(jnp.bfloat16)
    up_bf = up_weight.astype(jnp.bfloat16)
    down_bf = down_weight.astype(jnp.bfloat16)
    rep_index = lax.axis_index("rep")
    half_cols = gate_bf.shape[1] // 2
    half_rows = down_bf.shape[0] // 2
    own_gate = lax.dynamic_slice_in_dim(gate_bf, rep_index * half_cols, half_cols, 1)
    own_up = lax.dynamic_slice_in_dim(up_bf, rep_index * half_cols, half_cols, 1)
    own_down = lax.dynamic_slice_in_dim(down_bf, rep_index * half_rows, half_rows, 0)
    own_parts = (
        lax.all_gather(own_gate, "fs", axis=0, tiled=True),
        lax.all_gather(own_up, "fs", axis=0, tiled=True),
        lax.all_gather(own_down, "fs", axis=1, tiled=True),
    )
    far_parts = from_partner((own_parts[0], own_parts[1], own_parts[2]), "rep", 0)
    is_first = rep_index == 0

    def joined(own_part, far_part, axis_dim):
        return jnp.where(
            is_first,
            jnp.concatenate([own_part, far_part], axis_dim),
            jnp.concatenate([far_part, own_part], axis_dim),
        )

    gate_full = joined(own_parts[0], far_parts[0], 1)
    up_full = joined(own_parts[1], far_parts[1], 1)
    down_full = joined(own_parts[2], far_parts[2], 0)
    slab_rows = lax.all_gather(normed, "tp", axis=0, tiled=True)
    gate_pre = jnp.dot(slab_rows, gate_full, preferred_element_type=jnp.float32) * gate_scale
    up_pre = jnp.dot(slab_rows, up_full, preferred_element_type=jnp.float32) * up_scale
    hidden = (jax.nn.silu(gate_pre) * up_pre).astype(jnp.bfloat16)
    partial_value = (
        jnp.dot(hidden, down_full, preferred_element_type=jnp.float32) * down_scale
    ).astype(jnp.bfloat16)
    partial_value = lax.optimization_barrier(partial_value)
    return lax.psum_scatter(
        partial_value.astype(jnp.float32).astype(jnp.bfloat16),
        "tp",
        scatter_dimension=0,
        tiled=True,
    )


MESH = pl.DeviceIdType.MESH
CUTS = 4
DOWN = 2 * CUTS
PIECES = 4


def each(count, step):
    def go(index, carry):
        step(index)
        return carry

    lax.fori_loop(0, count, go, 0)


def ffn_kernel(
    tok_ref, gain_ref, gate_ref, gscale_ref, up_ref, uscale_ref, down_ref, dscale_ref, out_ref,
    tok, gain, gscale, uscale, dscale, raw_gu, raw_d, wgu, wd, tgu, td, scales, rows, acc, hid,
    staged, landed_x, summed, landed_z, landed_f, result,
    out_sem, px_send, px_recv, pz_send, pz_recv, pf_send,
):
    n_tok = tok.shape[0]
    piece_tok = n_tok // PIECES
    units = tgu.shape[3]
    depth = tgu.shape[2]
    fine = depth // CUTS
    cols = wd.shape[2]

    rep = lax.axis_index("rep")
    fs = lax.axis_index("fs")
    tp = lax.axis_index("tp")
    z = fs // 2
    y = fs % 2
    side_z = z // 2
    inner = (z + side_z) % 2
    outer = 1 - inner
    is_inner = inner == 1
    is_outer = inner == 0
    z_pair = 1 + 4 * side_z - z

    pair_dev = (rep, z_pair * 2 + y, tp)
    mid_dev = (rep, (3 - z) * 2 + y, tp)
    y_dev = (rep, z * 2 + 1 - y, tp)
    x_dev = (1 - rep, fs, tp)
    c_dev = (rep, fs, 1 - tp)

    def remote(src, dst, send, recv, device):
        return pltpu.make_async_remote_copy(
            src_ref=src, dst_ref=dst, send_sem=send, recv_sem=recv, device_id=device, device_id_type=MESH
        )

    def shard_z(turn):
        if isinstance(turn, int):
            return (z, z_pair, 2 - side_z, 3 - 3 * side_z)[turn]
        late = turn // 2
        odd = turn % 2
        early = (1 - odd) * z + odd * z_pair
        return (1 - late) * early + late * ((1 - odd) * (2 - side_z) + odd * (3 - 3 * side_z))

    def part_x(block, far):
        return remote(
            staged.at[block, far, 1], landed_x.at[block, far], px_send, px_recv.at[block, far], x_dev
        )

    def part_z(block):
        return remote(summed.at[block], landed_z.at[block], pz_send, pz_recv.at[block], pair_dev)

    def block_of(turn, side):
        return shard_z(turn) * 2 + y + side - 2 * side * y

    def z_first(turn, side):
        return ((turn < 2) & ((side == 1) | (turn + inner == 1))) | ((turn == 2) & (side == 0))

    def fold(turn, side):
        block = block_of(turn, side)

        @pl.when(is_inner | jnp.logical_not(z_first(turn, side)))
        def _():
            part_x(block, 1).wait_recv()
            total = staged[block, 1, 0].astype(jnp.float32) + landed_x[block, 1].astype(jnp.float32)
            summed[block] = total.astype(jnp.bfloat16)
            part_z(block).start()

    def out_copy(block):
        span = pl.ds(pl.multiple_of(block * cols, cols), cols)
        return pltpu.make_async_copy(result.at[:, span], out_ref.at[:, span], out_sem)

    def sent(src, send):
        remote(src, src, send, px_recv.at[0, 0], c_dev).wait_send()

    near = pl.ds(0, units)

    def phases(
        load_sem, scale_send, scale_recv, pair_send, mid_send, main_recv, thru_recv, y_send, y_recv, c_send, c_recv,
        tok_send, tok_recv, pf_recv,
    ):
        barrier = pltpu.get_barrier_semaphore()
        for device in (pair_dev, y_dev, x_dev, c_dev):
            pl.semaphore_signal(barrier, inc=1, device_id=device, device_id_type=MESH)

        @pl.when(is_inner)
        def _():
            pl.semaphore_signal(barrier, inc=1, device_id=mid_dev, device_id_type=MESH)

        def main_at(shard, shard_y, part, core):
            lanes = pl.ds(pl.multiple_of(core * units, 128), units)
            if isinstance(part, int) and part == DOWN:
                return wd.at[shard * 2 + shard_y, lanes]
            start = pl.multiple_of(shard_y * depth + (part % CUTS) * fine, fine)
            return wgu.at[part // CUTS, shard, pl.ds(start, fine), lanes]

        def thru_at(turn, part):
            if isinstance(part, int) and part == DOWN:
                return td.at[turn]
            start = pl.multiple_of((part % CUTS) * fine, fine)
            return tgu.at[part // CUTS, turn, pl.ds(start, fine)]

        def kind_of(part):
            return 1 if isinstance(part, int) and part == DOWN else 0

        def pair_copy(kind, part):
            send = pair_send.at[kind_of(part)]
            if kind == 0:
                return remote(thru_at(0, part), main_at(z, y, part, tp), send, main_recv.at[0, part], pair_dev)
            if kind == 1:
                return remote(main_at(z, y, part, tp), thru_at(1, part), send, thru_recv.at[0, part], pair_dev)
            return remote(
                thru_at(kind, part), main_at(shard_z(kind), y, part, tp), send, main_recv.at[kind - 1, part], pair_dev
            )

        def mid_copy(kind, part):
            send = mid_send.at[kind_of(part)]
            turn = 2 + kind // 2
            if kind % 2 == 0:
                ref = main_at(shard_z(kind // 2), y, part, tp)
                return remote(ref, ref, send, main_recv.at[turn - 1, part], mid_dev)
            return remote(thru_at(kind // 2, part), thru_at(turn, part), send, thru_recv.at[turn - 1, part], mid_dev)

        def main_in(turn, part):
            ref = main_at(shard_z(turn), y, part, tp)
            return remote(ref, ref, pair_send.at[0], main_recv.at[turn - 1, part], pair_dev)

        def thru_in(turn, part):
            ref = thru_at(turn, part)
            return remote(ref, ref, pair_send.at[0], thru_recv.at[turn - 1, part], pair_dev)

        def y_copy(turn, part):
            ref = main_at(shard_z(turn), y, part, tp)
            return remote(ref, ref, y_send.at[kind_of(part)], y_recv.at[turn, part], y_dev)

        def y_in(turn, part):
            ref = main_at(shard_z(turn), 1 - y, part, tp)
            return remote(ref, ref, y_send.at[kind_of(part)], y_recv.at[turn, part], y_dev)

        def c_copy(turn, side, part):
            ref = main_at(shard_z(turn), y + side - 2 * side * y, part, tp)
            return remote(ref, ref, c_send.at[kind_of(part)], c_recv.at[turn, side, kind_of(part)], c_dev)

        def c_in(turn, side, part):
            shard_y = y + side - 2 * side * y
            if part == DOWN:
                ref = main_at(shard_z(turn), shard_y, DOWN, 1 - tp)
            else:
                spare = pl.ds(pl.multiple_of((1 - tp) * units, 128), units)
                start = pl.multiple_of(shard_y * depth, depth)
                ref = wgu.at[:, shard_z(turn), pl.ds(start, depth), spare]
            return remote(ref, ref, c_send.at[kind_of(part)], c_recv.at[turn, side, kind_of(part)], c_dev)

        def tok_pair(piece):
            part = pl.ds(piece * piece_tok, piece_tok)
            return remote(
                rows.at[0, part], rows.at[1, part], tok_send.at[0], tok_recv.at[piece], pair_dev
            )

        def tok_far(piece):
            return remote(
                rows.at[1, pl.ds(piece * piece_tok, piece_tok)],
                rows.at[1, pl.ds(n_tok + piece * piece_tok, piece_tok)],
                tok_send.at[1], tok_recv.at[PIECES + piece], x_dev,
            )

        def tok_x():
            return remote(
                rows.at[0, pl.ds(0, n_tok)], rows.at[0, pl.ds(n_tok, n_tok)],
                tok_send.at[2], tok_recv.at[2 * PIECES], x_dev,
            )

        def early_z(block):
            return remote(staged.at[block, 1, 0], landed_z.at[block], pz_send, pz_recv.at[block], pair_dev)

        def place_of(turn, side):
            return side * (shard_z(turn) - 2 * side_z) + (1 - side) * (2 + turn // 2)

        def early_far(block, place):
            return remote(
                staged.at[block, 1, 1], landed_f.at[place], pf_send, pf_recv.at[place], pair_dev
            )

        def scale_copy():
            return remote(scales.at[tp], scales.at[tp], scale_send, scale_recv, c_dev)

        def scale_in():
            return remote(scales.at[1 - tp], scales.at[1 - tp], scale_send, scale_recv, c_dev)

        base = rep * 2 * units
        both = pl.ds(pl.multiple_of(base, 128), 2 * units)
        loads = []
        for part in range(DOWN):
            source = gate_ref if part // CUTS == 0 else up_ref
            span = pl.ds((part % CUTS) * fine, fine)
            loads.append((source.at[span, both], raw_gu.at[part // CUTS, span]))
        loads.append((down_ref.at[both], raw_d))
        loads += [(tok_ref, tok), (gain_ref, gain), (gscale_ref, gscale), (uscale_ref, uscale), (dscale_ref, dscale)]
        loads = [pltpu.make_async_copy(*pair, load_sem.at[index]) for index, pair in enumerate(loads)]
        for index in (0, 1, DOWN + 1, DOWN + 2, *range(2, DOWN + 1), DOWN + 3, DOWN + 4, DOWN + 5):
            loads[index].start()

        mine = pl.ds(pl.multiple_of(outer * units, 128), units)
        theirs = pl.ds(pl.multiple_of(inner * units, 128), units)
        lanes = pl.ds(pl.multiple_of(tp * units, 128), units)

        def round_part(part):
            loads[part].wait()
            span = slice((part % CUTS) * fine, (part % CUTS + 1) * fine)
            start = pl.multiple_of(y * depth + (part % CUTS) * fine, fine)
            wgu[part // CUTS, z, pl.ds(start, fine), lanes] = raw_gu[part // CUTS, span, mine].astype(jnp.bfloat16)
            tgu[part // CUTS, 0, span] = raw_gu[part // CUTS, span, theirs].astype(jnp.bfloat16)

        def send_part(part):
            pair_copy(0, part).start()
            y_copy(0, part).start()

            @pl.when(is_inner)
            def _():
                mid_copy(0, part).start()

            c_copy(0, 0, part).start()

        round_part(0)
        pl.semaphore_wait(barrier, 4 + inner)
        send_part(0)
        round_part(1)
        send_part(1)
        loads[DOWN + 1].wait()
        loads[DOWN + 2].wait()
        values = tok[...].astype(jnp.float32)
        inverse = lax.rsqrt(jnp.mean(values * values, axis=-1, keepdims=True) + EPS_VALUE)
        rows[0, :n_tok] = (values * inverse * gain[...]).astype(jnp.bfloat16)
        tok_x().start()
        for part in range(2, DOWN):
            round_part(part)
            send_part(part)
        for piece in range(PIECES):
            tok_pair(piece).start()

        @pl.when(is_inner)
        def _():
            each(DOWN, lambda part: mid_copy(1, part).start())

        @pl.when(is_outer)
        def _():
            each(DOWN, lambda part: pair_copy(1, part).start())

        for index in (DOWN + 3, DOWN + 4, DOWN + 5):
            loads[index].wait()
        first_row = (base + outer * units) // 128
        for index in range(units // 128):
            span = slice(index * 128, (index + 1) * 128)
            scales[tp, 0:1, span] = gscale[pl.ds(first_row + index, 1), :]
            scales[tp, 1:2, span] = uscale[pl.ds(first_row + index, 1), :]
        scale_copy().start()
        loads[DOWN].wait()
        wd[fs, lanes] = raw_d[mine].astype(jnp.bfloat16)
        td[0] = raw_d[theirs].astype(jnp.bfloat16)
        c_copy(0, 0, DOWN).start()

        @pl.when(is_outer)
        def _():
            pair_copy(0, DOWN).start()
            pair_copy(1, DOWN).start()

        def take_main(turn, part):
            main_in(turn, part).wait_recv()
            y_copy(turn, part).start()
            c_copy(turn, 0, part).start()

        def take_y(turn, part):
            y_in(turn, part).wait_recv()
            c_copy(turn, 1, part).start()

        def take_rows(piece):
            tok_pair(piece).wait_recv()
            tok_far(piece).start()

        def c_wait(turn):
            for side in range(2):
                c_in(turn, side, 0).wait_recv()

        def term(far, matrix, turn):
            shard = shard_z(turn)
            span = pl.ds(pl.multiple_of(shard * 2 * depth, 2 * depth), 2 * depth)
            return jnp.dot(rows[far, :, span], wgu[matrix, shard], preferred_element_type=jnp.float32)

        def add_early(part):
            far, matrix = part // 2, part % 2

            @pl.when(part == 2)
            def _():
                for piece in range(PIECES):
                    tok_far(piece).wait_recv()

            acc[matrix, far] = term(far, matrix, 0)
            acc[matrix, far] += term(far, matrix, 1)

        def add_late(part):
            acc[part % 2, part // 2] += term(part // 2, part % 2, 2)

        def half_term(far, matrix, span, side):
            shard = shard_z(3)
            shard_y = y + side - 2 * side * y
            start = pl.multiple_of((shard * 2 + shard_y) * depth, depth)
            inside = pl.multiple_of(shard_y * depth, depth)
            return jnp.dot(
                rows[far, span, pl.ds(start, depth)], wgu[matrix, shard, pl.ds(inside, depth)],
                preferred_element_type=jnp.float32,
            )

        def add_last(part):
            acc[part % 2, part // 2] += half_term(part // 2, part % 2, pl.ds(0, 2 * n_tok), 0)

        def first(part):
            take_main(1, part)

            @pl.when(is_inner)
            def _():
                mid_copy(2, part).start()

            take_y(0, part)

        each(DOWN, first)

        @pl.when(is_inner)
        def _():
            each(DOWN, lambda part: take_main(2, part))

        @pl.when(is_outer)
        def _():
            y_copy(0, DOWN).start()

        def second(part):
            @pl.when(is_inner)
            def _():
                thru_in(2, part).wait_recv()
                pair_copy(2, part).start()

            take_y(1, part)

            @pl.when((part == 3) | (part == 5))
            def _():
                take_rows((part - 3) // 2)

        each(DOWN, second)
        take_rows(2)

        def pass_outward(part):
            thru_in(1, part).wait_recv()
            mid_copy(3, part).start()

        @pl.when(is_inner)
        def _():
            def third(part):
                take_main(3, part)
                take_y(2, part)

                @pl.when(part == 3)
                def _():
                    take_rows(3)

                @pl.when(part > 5)
                def _():
                    pass_outward(part - 6)

            each(DOWN, third)
            y_copy(0, DOWN).start()

        @pl.when(is_outer)
        def _():
            take_rows(3)

        tok_x().wait_recv()
        c_wait(0)
        c_wait(1)

        @pl.when(is_inner)
        def _():
            c_wait(2)
            c_in(3, 0, 0).wait_recv()

            def fourth(chunk):
                @pl.when(chunk < 3)
                def _():
                    for ahead in (2, 3):
                        pass_outward(2 * chunk + ahead)

                @pl.when(chunk == 2)
                def _():
                    mid_copy(1, DOWN).start()
                    mid_copy(0, DOWN).start()

                add_early(chunk)
                add_late(chunk)
                for part in (2 * chunk, 2 * chunk + 1):
                    thru_in(3, part).wait_recv()
                    pair_copy(3, part).start()
                    take_y(3, part)
                add_last(chunk)

            each(4, fourth)
            pair_copy(0, DOWN).start()

        @pl.when(is_outer)
        def _():
            def fourth(chunk):
                for part in (2 * chunk, 2 * chunk + 1):
                    take_main(2, part)

                    @pl.when(chunk > 0)
                    def _():
                        take_y(2, part - 2)

                add_early(chunk)

            each(4, fourth)

            def fifth(chunk):
                for part in (2 * chunk, 2 * chunk + 1):
                    take_main(3, part)

                    @pl.when(chunk == 0)
                    def _():
                        take_y(2, part + 6)

                    @pl.when(chunk > 0)
                    def _():
                        take_y(3, part - 2)

                @pl.when(chunk == 0)
                def _():
                    c_wait(2)

                add_late(chunk)

            each(4, fifth)
            c_in(3, 0, 0).wait_recv()
            take_y(3, 6)
            each(2, add_last)
            take_y(3, 7)
            each(2, lambda chunk: add_last(chunk + 2))
            take_y(0, DOWN)
            c_in(0, 1, DOWN).wait_recv()

        def send_off(turn, side, far, near_x):
            block = block_of(turn, side)
            ahead = z_first(turn, side)
            crossing = far + inner == 1

            held = is_outer & (turn == 2) & (side == 1) & (far == 0)

            @pl.when((near_x == 1) & jnp.logical_not((ahead & crossing) | held))
            def _():
                part_x(block, far).start()

            @pl.when(ahead & crossing & is_outer)
            def _():
                @pl.when(near_x == 1)
                def _():
                    early_far(block, place_of(turn, side)).start()

                @pl.when(near_x == 0)
                def _():
                    early_z(block).start()

        def scale_of(block):
            return dscale[:, pl.ds(pl.multiple_of(block * cols, cols), cols)]

        scale_in().wait_recv()
        c_in(3, 1, 0).wait_recv()
        c_in(0, 0, DOWN).wait_recv()

        def activate(index):
            far = 1 - index % 2
            near_x = 1 - index // 2
            span = pl.ds(pl.multiple_of(near_x * n_tok, n_tok), n_tok)
            pre = []

            @pl.when(index == 1 + inner)
            def _():
                take_main(1, DOWN)

            for matrix in range(2):
                last = half_term(far, matrix, span, 1)
                scale = jnp.concatenate(
                    [scales[0, matrix:matrix + 1], scales[1, matrix:matrix + 1]], axis=1
                )
                pre.append((acc[matrix, far, span] + last) * scale)
            hid[far, span] = (jax.nn.silu(pre[0]) * pre[1]).astype(jnp.bfloat16)

            def one(side, carry):
                block = block_of(0, side)
                product = jnp.dot(hid[far, span], wd[block], preferred_element_type=jnp.float32) * scale_of(block)
                staged[block, far, near_x] = product.astype(jnp.bfloat16)
                send_off(0, side, far, near_x)
                return carry

            lax.fori_loop(0, 1 + outer, one, 0)

        each(4, activate)

        def produce(turn, side):
            block = block_of(turn, side)

            def tile(index):
                far = 1 - index
                product = jnp.dot(hid[far], wd[block], preferred_element_type=jnp.float32) * scale_of(block)
                staged[block, far] = product.astype(jnp.bfloat16).reshape(2, n_tok, cols)
                for near_x in (1, 0):
                    send_off(turn, side, far, near_x)

            each(2, tile)

        def late_x(turn, side):
            block = block_of(turn, side)
            place = place_of(turn, side)
            early_far(block, place).wait_recv()
            total = staged[block, 0, 1].astype(jnp.float32) + landed_f[place].astype(jnp.float32)
            staged[block, 0, 1] = total.astype(jnp.bfloat16)
            part_x(block, 0).start()

        def down_step(index):
            step = index + 1
            swap = inner * (step // 3) * (1 - step // 4)

            @pl.when(is_inner & (step == 2))
            def _():
                take_main(2, DOWN)

            @pl.when(is_inner & (step == 4))
            def _():
                late_x(0, 0)

            @pl.when(is_inner | (step > 1))
            def _():
                take_y(step - 1, DOWN)

            def sides(order):
                side = order + swap - 2 * order * swap
                turn = step - side

                @pl.when((turn < 4) & ((side == 0) | (turn > 0) | is_inner))
                def _():
                    @pl.when(is_inner & (side == 0) & (turn == 3))
                    def _():
                        late_x(1, 1)
                        take_main(3, DOWN)

                    c_in(turn, side, DOWN).wait_recv()
                    produce(turn, side)

            each(2, sides)

            @pl.when(is_inner)
            def _():
                @pl.when(step == 1)
                def _():
                    thru_in(2, DOWN).wait_recv()
                    pair_copy(2, DOWN).start()
                    thru_in(1, DOWN).wait_recv()
                    mid_copy(3, DOWN).start()
                    mid_copy(2, DOWN).start()

                @pl.when(step == 2)
                def _():
                    thru_in(3, DOWN).wait_recv()
                    pair_copy(3, DOWN).start()

                @pl.when(step == 4)
                def _():
                    late_x(0, 1)

            @pl.when(is_outer & (step < 3))
            def _():
                take_main(step + 1, DOWN)

            @pl.when(is_outer & (step == 4))
            def _():
                part_x(block_of(2, 1), 0).start()

            def folds(side):
                @pl.when(step - 1 - side >= 0)
                def _():
                    fold(step - 1 - side, side)

            each(2, folds)

        each(4, down_step)


        @pl.when(is_inner)
        def _():
            late_x(2, 0)

        def drain(turns, pair_turns):
            for count, send in ((pair_turns, pair_send), (turns, mid_send)):
                if count:
                    sent(wgu.at[:, pl.ds(0, count), pl.ds(0, depth), near], send.at[0])
                    sent(wd.at[pl.ds(0, count), near], send.at[1])

        @pl.when(is_inner)
        def _():
            drain(4, 3)

        @pl.when(is_outer)
        def _():
            drain(0, 2)

        sent(wgu.at[:, :, pl.ds(0, depth), near], y_send.at[0])
        sent(wd.at[pl.ds(0, 4), near], y_send.at[1])
        sent(wgu.at[:, :, :, near], c_send.at[0])
        sent(wd.at[:, near], c_send.at[1])
        for index in range(3):
            sent(rows.at[0, pl.ds(0, n_tok)], tok_send.at[index])
        scale_copy().wait_send()

    dma = pltpu.SemaphoreType.DMA
    turns, parts = 4, DOWN + 1
    pl.run_scoped(
        phases,
        dma((DOWN + 6,)), dma, dma, dma((2,)), dma((2,)), dma((turns - 1, parts)), dma((turns - 1, parts)),
        dma((2,)), dma((turns, parts)), dma((2,)), dma((turns, 2, 2)), dma((3,)), dma((2 * PIECES + 1,)),
        dma((4,)),
    )
    fold(3, 1)

    def finish(index):
        block = block_of(outer * (index // 2) + inner * (3 - index // 2), index % 2)
        part_x(block, 0).wait_recv()
        part_z(block).wait_recv()
        total = staged[block, 0, 0].astype(jnp.float32) + landed_x[block, 0].astype(jnp.float32)
        total = total + landed_z[block].astype(jnp.float32)
        result[:, pl.ds(pl.multiple_of(block * cols, cols), cols)] = total.astype(result.dtype)
        out_copy(block).start()

    each(8, finish)

    sent(landed_z, pz_send)

    @pl.when(is_inner)
    def _():
        sent(staged.at[pl.ds(0, 4)], px_send)

    @pl.when(is_outer)
    def _():
        sent(staged.at[pl.ds(0, 3)], px_send)
        sent(staged.at[0], pf_send)

    pltpu.make_async_copy(result, out_ref, out_sem).wait()


def kernel_body(tokens, norm_gain, gate_weight, gate_scale, up_weight, up_scale, down_weight, down_scale, sizes):
    n_fs = sizes[1]
    n_tok, width = tokens.shape
    depth = gate_weight.shape[0]
    all_units = gate_weight.shape[1]
    units = all_units // (2 * sizes[0])
    cols = down_weight.shape[1]
    anywhere = pl.BlockSpec(memory_space=pl.ANY)
    bf, wide = jnp.bfloat16, jnp.float32
    dma = pltpu.SemaphoreType.DMA
    turns = 4
    return pl.pallas_call(
        ffn_kernel,
        out_shape=jax.ShapeDtypeStruct((n_tok, width), bf),
        in_specs=[anywhere] * 8,
        out_specs=anywhere,
        scratch_shapes=[
            pltpu.VMEM((n_tok, width), bf),
            pltpu.VMEM((1, width), wide),
            pltpu.VMEM((all_units // 128, 128), wide),
            pltpu.VMEM((all_units // 128, 128), wide),
            pltpu.VMEM((1, width), wide),
            pltpu.VMEM((2, depth, 2 * units), wide),
            pltpu.VMEM((2 * units, cols), wide),
            pltpu.VMEM((2, n_fs // 2, 2 * depth, 2 * units), bf),
            pltpu.VMEM((n_fs, 2 * units, cols), bf),
            pltpu.VMEM((2, turns, depth, units), bf),
            pltpu.VMEM((turns, units, cols), bf),
            pltpu.VMEM((2, 2, units), wide),
            pltpu.VMEM((2, 2 * n_tok, width), bf),
            pltpu.VMEM((2, 2, 2 * n_tok, 2 * units), wide),
            pltpu.VMEM((2, 2 * n_tok, 2 * units), bf),
            pltpu.VMEM((n_fs, 2, 2, n_tok, cols), bf),
            pltpu.VMEM((n_fs, 2, n_tok, cols), bf),
            pltpu.VMEM((n_fs, n_tok, cols), bf),
            pltpu.VMEM((n_fs, n_tok, cols), bf),
            pltpu.VMEM((4, n_tok, cols), bf),
            pltpu.VMEM((n_tok, width), bf),
            dma, dma, dma((n_fs, 2)), dma, dma((n_fs,)), dma,
        ],
        compiler_params=pltpu.CompilerParams(
            collective_id=0, has_side_effects=True, vmem_limit_bytes=62 * 1024 * 1024
        ),
    )(
        tokens, norm_gain[None, :], gate_weight, gate_scale.reshape(-1, 128), up_weight, up_scale.reshape(-1, 128),
        down_weight, down_scale[None, :],
    )


def fits_kernel(mesh, tokens, gate_weight, down_weight):
    n_rep, n_fs, n_tp = (mesh.shape[name] for name in ("rep", "fs", "tp"))
    units = gate_weight.shape[1] // (n_tp * n_rep * 2)
    aligned = units % 128 == 0 and down_weight.shape[1] // n_fs % 128 == 0
    aligned = aligned and gate_weight.shape[0] // n_fs % (32 * CUTS) == 0
    return aligned and n_rep == 2 and n_fs == 8 and n_tp == 2


def solution(mesh):
    sizes = tuple(mesh.shape[name] for name in ("rep", "fs", "tp"))

    def run(tokens, norm_gain, gate_weight, gate_scale, up_weight, up_scale, down_weight, down_scale):
        chosen = body
        if fits_kernel(mesh, tokens, gate_weight, down_weight):
            chosen = functools.partial(kernel_body, sizes=sizes)
        return jax.shard_map(
            chosen,
            mesh=mesh,
            in_specs=(
                P(("rep", "fs", "tp"), None),
                P(),
                P("fs", "tp"),
                P("tp"),
                P("fs", "tp"),
                P("tp"),
                P("tp", "fs"),
                P(),
            ),
            out_specs=P(("rep", "fs", "tp"), None),
            check_vma=False,
        )(tokens, norm_gain, gate_weight, gate_scale, up_weight, up_scale, down_weight, down_scale)

    return run
```

```python
import functools

import jax
import jax.numpy as jnp
from jax import lax
from jax.experimental import pallas as pl
from jax.experimental.pallas import tpu as pltpu
from jax.sharding import PartitionSpec as P

EPS_VALUE = 1e-06


def from_partner(shard, axis, distance):
    return lax.ppermute(shard, axis, [(i, i ^ 1 << distance) for i in range(lax.axis_size(axis))])


def normalize(token_rows, norm_gain):
    values = token_rows.astype(jnp.float32)
    inverse = lax.rsqrt(jnp.mean(values * values, axis=-1, keepdims=True) + EPS_VALUE)
    return (values * inverse * norm_gain).astype(jnp.bfloat16)


def body(tokens, norm_gain, gate_weight, gate_scale, up_weight, up_scale, down_weight, down_scale):
    normed = normalize(tokens, norm_gain)
    gate_bf = gate_weight.astype(jnp.bfloat16)
    up_bf = up_weight.astype(jnp.bfloat16)
    down_bf = down_weight.astype(jnp.bfloat16)
    rep_index = lax.axis_index("rep")
    half_cols = gate_bf.shape[1] // 2
    half_rows = down_bf.shape[0] // 2
    own_gate = lax.dynamic_slice_in_dim(gate_bf, rep_index * half_cols, half_cols, 1)
    own_up = lax.dynamic_slice_in_dim(up_bf, rep_index * half_cols, half_cols, 1)
    own_down = lax.dynamic_slice_in_dim(down_bf, rep_index * half_rows, half_rows, 0)
    own_parts = (
        lax.all_gather(own_gate, "fs", axis=0, tiled=True),
        lax.all_gather(own_up, "fs", axis=0, tiled=True),
        lax.all_gather(own_down, "fs", axis=1, tiled=True),
    )
    far_parts = from_partner((own_parts[0], own_parts[1], own_parts[2]), "rep", 0)
    is_first = rep_index == 0

    def joined(own_part, far_part, axis_dim):
        return jnp.where(
            is_first,
            jnp.concatenate([own_part, far_part], axis_dim),
            jnp.concatenate([far_part, own_part], axis_dim),
        )

    gate_full = joined(own_parts[0], far_parts[0], 1)
    up_full = joined(own_parts[1], far_parts[1], 1)
    down_full = joined(own_parts[2], far_parts[2], 0)
    slab_rows = lax.all_gather(normed, "tp", axis=0, tiled=True)
    gate_pre = jnp.dot(slab_rows, gate_full, preferred_element_type=jnp.float32) * gate_scale
    up_pre = jnp.dot(slab_rows, up_full, preferred_element_type=jnp.float32) * up_scale
    hidden = (jax.nn.silu(gate_pre) * up_pre).astype(jnp.bfloat16)
    partial_value = (
        jnp.dot(hidden, down_full, preferred_element_type=jnp.float32) * down_scale
    ).astype(jnp.bfloat16)
    partial_value = lax.optimization_barrier(partial_value)
    return lax.psum_scatter(
        partial_value.astype(jnp.float32).astype(jnp.bfloat16),
        "tp",
        scatter_dimension=0,
        tiled=True,
    )


MESH = pl.DeviceIdType.MESH
CUTS = 8
DOWN = 2 * CUTS
QUARTER = DOWN // 4
PIECES = 4


def each(count, step):
    def go(index, carry):
        step(index)
        return carry

    lax.fori_loop(0, count, go, 0)


def ffn_kernel(
    tok_ref, gain_ref, gate_ref, gscale_ref, up_ref, uscale_ref, down_ref, dscale_ref, out_ref,
    tok, gain, gscale, uscale, dscale, raw_gu, raw_d, wgu, wd, tgu, td, scales, rows, acc, hid,
    staged, landed_x, summed, landed_z, landed_f, result,
    out_sem, px_send, px_recv, pz_send, pz_recv, pf_send,
):
    n_tok = tok.shape[0]
    piece_tok = n_tok // PIECES
    units = tgu.shape[3]
    depth = tgu.shape[2]
    fine = depth // CUTS
    cols = wd.shape[2]

    rep = lax.axis_index("rep")
    fs = lax.axis_index("fs")
    tp = lax.axis_index("tp")
    z = fs // 2
    y = fs % 2
    side_z = z // 2
    inner = (z + side_z) % 2
    outer = 1 - inner
    is_inner = inner == 1
    is_outer = inner == 0
    z_pair = 1 + 4 * side_z - z

    pair_dev = (rep, z_pair * 2 + y, tp)
    mid_dev = (rep, (3 - z) * 2 + y, tp)
    y_dev = (rep, z * 2 + 1 - y, tp)
    x_dev = (1 - rep, fs, tp)
    c_dev = (rep, fs, 1 - tp)

    def remote(src, dst, send, recv, device):
        return pltpu.make_async_remote_copy(
            src_ref=src, dst_ref=dst, send_sem=send, recv_sem=recv, device_id=device, device_id_type=MESH
        )

    def shard_z(turn):
        if isinstance(turn, int):
            return (z, z_pair, 2 - side_z, 3 - 3 * side_z)[turn]
        late = turn // 2
        odd = turn % 2
        early = (1 - odd) * z + odd * z_pair
        return (1 - late) * early + late * ((1 - odd) * (2 - side_z) + odd * (3 - 3 * side_z))

    def part_x(block, far):
        return remote(
            staged.at[block, far, 1], landed_x.at[block, far], px_send, px_recv.at[block, far], x_dev
        )

    def part_z(block):
        return remote(summed.at[block], landed_z.at[block], pz_send, pz_recv.at[block], pair_dev)

    def block_of(turn, side):
        return shard_z(turn) * 2 + y + side - 2 * side * y

    def z_first(turn, side):
        return ((turn < 2) & ((side == 1) | (turn + inner == 1))) | ((turn == 3) & (side == 0))

    def fold(turn, side):
        block = block_of(turn, side)

        @pl.when(is_inner | jnp.logical_not(z_first(turn, side)))
        def _():
            part_x(block, 1).wait_recv()
            total = staged[block, 1, 0].astype(jnp.float32) + landed_x[block, 1].astype(jnp.float32)
            summed[block] = total.astype(jnp.bfloat16)
            part_z(block).start()

    def out_copy(block):
        span = pl.ds(pl.multiple_of(block * cols, cols), cols)
        return pltpu.make_async_copy(result.at[:, span], out_ref.at[:, span], out_sem)

    def sent(src, send):
        remote(src, src, send, px_recv.at[0, 0], c_dev).wait_send()

    near = pl.ds(0, units)

    def phases(
        load_sem, scale_send, scale_recv, pair_send, mid_send, main_recv, thru_recv, y_send, y_recv, c_send, c_recv,
        tok_send, tok_recv, pf_recv,
    ):
        barrier = pltpu.get_barrier_semaphore()
        for device in (pair_dev, y_dev, x_dev, c_dev):
            pl.semaphore_signal(barrier, inc=1, device_id=device, device_id_type=MESH)

        @pl.when(is_inner)
        def _():
            pl.semaphore_signal(barrier, inc=1, device_id=mid_dev, device_id_type=MESH)

        def main_at(shard, shard_y, part, core):
            lanes = pl.ds(pl.multiple_of(core * units, 128), units)
            if isinstance(part, int) and part == DOWN:
                return wd.at[shard * 2 + shard_y, lanes]
            start = pl.multiple_of(shard_y * depth + (part % CUTS) * fine, fine)
            return wgu.at[part // CUTS, shard, pl.ds(start, fine), lanes]

        def thru_at(turn, part):
            if isinstance(part, int) and part == DOWN:
                return td.at[turn]
            start = pl.multiple_of((part % CUTS) * fine, fine)
            return tgu.at[part // CUTS, turn, pl.ds(start, fine)]

        def kind_of(part):
            return 1 if isinstance(part, int) and part == DOWN else 0

        def pair_copy(kind, part):
            send = pair_send.at[kind_of(part)]
            if kind == 0:
                return remote(thru_at(0, part), main_at(z, y, part, tp), send, main_recv.at[0, part], pair_dev)
            if kind == 1:
                return remote(main_at(z, y, part, tp), thru_at(1, part), send, thru_recv.at[0, part], pair_dev)
            return remote(
                thru_at(kind, part), main_at(shard_z(kind), y, part, tp), send, main_recv.at[kind - 1, part], pair_dev
            )

        def mid_copy(kind, part):
            send = mid_send.at[kind_of(part)]
            turn = 2 + kind // 2
            if kind % 2 == 0:
                ref = main_at(shard_z(kind // 2), y, part, tp)
                return remote(ref, ref, send, main_recv.at[turn - 1, part], mid_dev)
            return remote(thru_at(kind // 2, part), thru_at(turn, part), send, thru_recv.at[turn - 1, part], mid_dev)

        def main_in(turn, part):
            ref = main_at(shard_z(turn), y, part, tp)
            return remote(ref, ref, pair_send.at[0], main_recv.at[turn - 1, part], pair_dev)

        def thru_in(turn, part):
            ref = thru_at(turn, part)
            return remote(ref, ref, pair_send.at[0], thru_recv.at[turn - 1, part], pair_dev)

        def y_copy(turn, part):
            ref = main_at(shard_z(turn), y, part, tp)
            return remote(ref, ref, y_send.at[kind_of(part)], y_recv.at[turn, part], y_dev)

        def y_in(turn, part):
            ref = main_at(shard_z(turn), 1 - y, part, tp)
            return remote(ref, ref, y_send.at[kind_of(part)], y_recv.at[turn, part], y_dev)

        def c_copy(turn, side, part):
            ref = main_at(shard_z(turn), y + side - 2 * side * y, part, tp)
            return remote(ref, ref, c_send.at[kind_of(part)], c_recv.at[turn, side, kind_of(part)], c_dev)

        def c_in(turn, side, part):
            shard_y = y + side - 2 * side * y
            if part == DOWN:
                ref = main_at(shard_z(turn), shard_y, DOWN, 1 - tp)
            else:
                spare = pl.ds(pl.multiple_of((1 - tp) * units, 128), units)
                start = pl.multiple_of(shard_y * depth, depth)
                ref = wgu.at[:, shard_z(turn), pl.ds(start, depth), spare]
            return remote(ref, ref, c_send.at[kind_of(part)], c_recv.at[turn, side, kind_of(part)], c_dev)

        def tok_pair(piece):
            part = pl.ds(piece * piece_tok, piece_tok)
            return remote(
                rows.at[0, part], rows.at[1, part], tok_send.at[0], tok_recv.at[piece], pair_dev
            )

        def tok_far(piece):
            return remote(
                rows.at[1, pl.ds(piece * piece_tok, piece_tok)],
                rows.at[1, pl.ds(n_tok + piece * piece_tok, piece_tok)],
                tok_send.at[1], tok_recv.at[PIECES + piece], x_dev,
            )

        def tok_x():
            return remote(
                rows.at[0, pl.ds(0, n_tok)], rows.at[0, pl.ds(n_tok, n_tok)],
                tok_send.at[2], tok_recv.at[2 * PIECES], x_dev,
            )

        def early_z(block):
            return remote(staged.at[block, 1, 0], landed_z.at[block], pz_send, pz_recv.at[block], pair_dev)

        def place_of(turn, side):
            return side * (shard_z(turn) - 2 * side_z) + (1 - side) * (2 + turn // 2)

        def early_far(block, place):
            return remote(
                staged.at[block, 1, 1], landed_f.at[place], pf_send, pf_recv.at[place], pair_dev
            )

        def scale_copy():
            return remote(scales.at[tp], scales.at[tp], scale_send, scale_recv, c_dev)

        def scale_in():
            return remote(scales.at[1 - tp], scales.at[1 - tp], scale_send, scale_recv, c_dev)

        base = rep * 2 * units
        both = pl.ds(pl.multiple_of(base, 128), 2 * units)
        loads = []
        for part in range(DOWN):
            source = gate_ref if part // CUTS == 0 else up_ref
            span = pl.ds((part % CUTS) * fine, fine)
            loads.append((source.at[span, both], raw_gu.at[part // CUTS, span]))
        loads.append((down_ref.at[both], raw_d))
        loads += [(tok_ref, tok), (gain_ref, gain), (gscale_ref, gscale), (uscale_ref, uscale), (dscale_ref, dscale)]
        loads = [pltpu.make_async_copy(*pair, load_sem.at[index]) for index, pair in enumerate(loads)]
        for index in (0, 1, DOWN + 1, DOWN + 2, *range(2, DOWN + 1), DOWN + 3, DOWN + 4, DOWN + 5):
            loads[index].start()

        mine = pl.ds(pl.multiple_of(outer * units, 128), units)
        theirs = pl.ds(pl.multiple_of(inner * units, 128), units)
        lanes = pl.ds(pl.multiple_of(tp * units, 128), units)

        def round_part(part):
            loads[part].wait()
            span = slice((part % CUTS) * fine, (part % CUTS + 1) * fine)
            start = pl.multiple_of(y * depth + (part % CUTS) * fine, fine)
            wgu[part // CUTS, z, pl.ds(start, fine), lanes] = raw_gu[part // CUTS, span, mine].astype(jnp.bfloat16)
            tgu[part // CUTS, 0, span] = raw_gu[part // CUTS, span, theirs].astype(jnp.bfloat16)

        def send_part(part):
            pair_copy(0, part).start()
            y_copy(0, part).start()

            @pl.when(is_inner)
            def _():
                mid_copy(0, part).start()

            c_copy(0, 0, part).start()

        round_part(0)
        pl.semaphore_wait(barrier, 4 + inner)
        send_part(0)
        round_part(1)
        send_part(1)
        loads[DOWN + 1].wait()
        loads[DOWN + 2].wait()
        values = tok[...].astype(jnp.float32)
        inverse = lax.rsqrt(jnp.mean(values * values, axis=-1, keepdims=True) + EPS_VALUE)
        rows[0, :n_tok] = (values * inverse * gain[...]).astype(jnp.bfloat16)
        tok_x().start()
        for part in range(2, DOWN):
            round_part(part)
            send_part(part)
        for piece in range(PIECES):
            tok_pair(piece).start()

        @pl.when(is_inner)
        def _():
            each(DOWN, lambda part: mid_copy(1, part).start())

        @pl.when(is_outer)
        def _():
            each(DOWN, lambda part: pair_copy(1, part).start())

        for index in (DOWN + 3, DOWN + 4, DOWN + 5):
            loads[index].wait()
        first_row = (base + outer * units) // 128
        for index in range(units // 128):
            span = slice(index * 128, (index + 1) * 128)
            scales[tp, 0:1, span] = gscale[pl.ds(first_row + index, 1), :]
            scales[tp, 1:2, span] = uscale[pl.ds(first_row + index, 1), :]
        scale_copy().start()
        loads[DOWN].wait()
        wd[fs, lanes] = raw_d[mine].astype(jnp.bfloat16)
        td[0] = raw_d[theirs].astype(jnp.bfloat16)
        c_copy(0, 0, DOWN).start()

        @pl.when(is_outer)
        def _():
            pair_copy(0, DOWN).start()
            pair_copy(1, DOWN).start()

        def take_main(turn, part):
            main_in(turn, part).wait_recv()
            y_copy(turn, part).start()
            c_copy(turn, 0, part).start()

        def take_y(turn, part):
            y_in(turn, part).wait_recv()
            c_copy(turn, 1, part).start()

        def take_rows(piece):
            tok_pair(piece).wait_recv()
            tok_far(piece).start()

        def c_wait(turn):
            for side in range(2):
                c_in(turn, side, 0).wait_recv()

        def term(far, matrix, turn):
            shard = shard_z(turn)
            span = pl.ds(pl.multiple_of(shard * 2 * depth, 2 * depth), 2 * depth)
            return jnp.dot(rows[far, :, span], wgu[matrix, shard], preferred_element_type=jnp.float32)

        def add_early(part):
            far, matrix = part // 2, part % 2

            @pl.when(part == 2)
            def _():
                for piece in range(PIECES):
                    tok_far(piece).wait_recv()

            acc[matrix, far] = term(far, matrix, 0)
            acc[matrix, far] += term(far, matrix, 1)

        def add_late(part):
            acc[part % 2, part // 2] += term(part // 2, part % 2, 2)

        def half_term(far, matrix, span, side):
            shard = shard_z(3)
            shard_y = y + side - 2 * side * y
            start = pl.multiple_of((shard * 2 + shard_y) * depth, depth)
            inside = pl.multiple_of(shard_y * depth, depth)
            return jnp.dot(
                rows[far, span, pl.ds(start, depth)], wgu[matrix, shard, pl.ds(inside, depth)],
                preferred_element_type=jnp.float32,
            )

        def add_last(part):
            acc[part % 2, part // 2] += half_term(part // 2, part % 2, pl.ds(0, 2 * n_tok), 0)

        def first(part):
            take_main(1, part)

            @pl.when(is_inner)
            def _():
                mid_copy(2, part).start()

            take_y(0, part)

        each(DOWN, first)

        @pl.when(is_inner)
        def _():
            each(DOWN, lambda part: take_main(2, part))

        @pl.when(is_outer)
        def _():
            y_copy(0, DOWN).start()

        def second(part):
            @pl.when(is_inner)
            def _():
                thru_in(2, part).wait_recv()
                pair_copy(2, part).start()

            take_y(1, part)

            for piece in range(2):
                @pl.when(part == QUARTER * (piece + 2) - 1)
                def _():
                    take_rows(piece)

        each(DOWN, second)
        take_rows(2)

        def pass_outward(part):
            thru_in(1, part).wait_recv()
            mid_copy(3, part).start()

        @pl.when(is_inner)
        def _():
            def third(part):
                take_main(3, part)
                take_y(2, part)

                @pl.when(part == 2 * QUARTER - 1)
                def _():
                    take_rows(3)

                @pl.when(part >= 3 * QUARTER)
                def _():
                    pass_outward(part - 3 * QUARTER)

            each(DOWN, third)
            y_copy(0, DOWN).start()

        @pl.when(is_outer)
        def _():
            take_rows(3)

        tok_x().wait_recv()
        c_wait(0)
        c_wait(1)

        @pl.when(is_inner)
        def _():
            c_wait(2)
            c_in(3, 0, 0).wait_recv()

            def fourth(chunk):
                @pl.when(chunk < 3)
                def _():
                    for ahead in range(QUARTER):
                        pass_outward(QUARTER * (chunk + 1) + ahead)

                @pl.when(chunk == 2)
                def _():
                    mid_copy(1, DOWN).start()
                    mid_copy(0, DOWN).start()

                add_early(chunk)
                add_late(chunk)
                for part in [QUARTER * chunk + index for index in range(QUARTER)]:
                    thru_in(3, part).wait_recv()
                    pair_copy(3, part).start()
                    take_y(3, part)
                add_last(chunk)

            each(4, fourth)
            pair_copy(0, DOWN).start()

        @pl.when(is_outer)
        def _():
            def fourth(chunk):
                for part in [QUARTER * chunk + index for index in range(QUARTER)]:
                    take_main(2, part)

                    @pl.when(chunk > 0)
                    def _():
                        take_y(2, part - QUARTER)

                add_early(chunk)

            each(4, fourth)

            def fifth(chunk):
                for part in [QUARTER * chunk + index for index in range(QUARTER)]:
                    take_main(3, part)

                    @pl.when(chunk == 0)
                    def _():
                        take_y(2, part + DOWN - QUARTER)

                    @pl.when(chunk > 0)
                    def _():
                        take_y(3, part - QUARTER)

                @pl.when(chunk == 0)
                def _():
                    c_wait(2)

                add_late(chunk)

            each(4, fifth)
            c_in(3, 0, 0).wait_recv()
            for part in range(QUARTER // 2):
                take_y(3, DOWN - QUARTER + part)
            each(2, add_last)
            for part in range(QUARTER // 2, QUARTER):
                take_y(3, DOWN - QUARTER + part)
            each(2, lambda chunk: add_last(chunk + 2))
            take_y(0, DOWN)
            c_in(0, 1, DOWN).wait_recv()

        def send_off(turn, side, far, near_x):
            block = block_of(turn, side)
            ahead = z_first(turn, side)
            crossing = far + inner == 1

            held = is_outer & (turn == 2) & (side == 1) & (far == 0)

            @pl.when((near_x == 1) & jnp.logical_not((ahead & crossing) | held))
            def _():
                part_x(block, far).start()

            @pl.when(ahead & crossing & is_outer)
            def _():
                @pl.when(near_x == 1)
                def _():
                    early_far(block, place_of(turn, side)).start()

                @pl.when(near_x == 0)
                def _():
                    early_z(block).start()

        def scale_of(block):
            return dscale[:, pl.ds(pl.multiple_of(block * cols, cols), cols)]

        scale_in().wait_recv()
        c_in(3, 1, 0).wait_recv()
        c_in(0, 0, DOWN).wait_recv()

        def activate(index):
            far = 1 - index % 2
            near_x = 1 - index // 2
            span = pl.ds(pl.multiple_of(near_x * n_tok, n_tok), n_tok)
            pre = []

            @pl.when(index == 1 + inner)
            def _():
                take_main(1, DOWN)

            for matrix in range(2):
                last = half_term(far, matrix, span, 1)
                scale = jnp.concatenate(
                    [scales[0, matrix:matrix + 1], scales[1, matrix:matrix + 1]], axis=1
                )
                pre.append((acc[matrix, far, span] + last) * scale)
            hid[far, span] = (jax.nn.silu(pre[0]) * pre[1]).astype(jnp.bfloat16)

            def one(side, carry):
                block = block_of(0, side)
                product = jnp.dot(hid[far, span], wd[block], preferred_element_type=jnp.float32) * scale_of(block)
                staged[block, far, near_x] = product.astype(jnp.bfloat16)
                send_off(0, side, far, near_x)
                return carry

            lax.fori_loop(0, 1 + outer, one, 0)

        each(4, activate)

        def produce(turn, side):
            block = block_of(turn, side)

            def tile(index):
                far = 1 - index
                product = jnp.dot(hid[far], wd[block], preferred_element_type=jnp.float32) * scale_of(block)
                staged[block, far] = product.astype(jnp.bfloat16).reshape(2, n_tok, cols)
                for near_x in (1, 0):
                    send_off(turn, side, far, near_x)

            each(2, tile)

        def late_x(turn, side):
            block = block_of(turn, side)
            place = place_of(turn, side)
            early_far(block, place).wait_recv()
            total = staged[block, 0, 1].astype(jnp.float32) + landed_f[place].astype(jnp.float32)
            staged[block, 0, 1] = total.astype(jnp.bfloat16)
            part_x(block, 0).start()

        def down_step(index):
            step = index + 1
            swap = inner * (step // 3) * (1 - step // 4)

            @pl.when(is_inner & (step == 2))
            def _():
                take_main(2, DOWN)

            @pl.when(is_inner & (step == 4))
            def _():
                late_x(0, 0)

            @pl.when(is_inner | (step > 1))
            def _():
                take_y(step - 1, DOWN)

            def sides(order):
                side = order + swap - 2 * order * swap
                turn = step - side

                @pl.when((turn < 4) & ((side == 0) | (turn > 0) | is_inner))
                def _():
                    @pl.when(is_inner & (side == 0) & (turn == 3))
                    def _():
                        late_x(1, 1)
                        take_main(3, DOWN)

                    c_in(turn, side, DOWN).wait_recv()
                    produce(turn, side)

            each(2, sides)

            @pl.when(is_inner)
            def _():
                @pl.when(step == 1)
                def _():
                    thru_in(2, DOWN).wait_recv()
                    pair_copy(2, DOWN).start()
                    thru_in(1, DOWN).wait_recv()
                    mid_copy(3, DOWN).start()
                    mid_copy(2, DOWN).start()

                @pl.when(step == 2)
                def _():
                    thru_in(3, DOWN).wait_recv()
                    pair_copy(3, DOWN).start()

                @pl.when(step == 4)
                def _():
                    late_x(0, 1)

            @pl.when(is_outer & (step < 3))
            def _():
                take_main(step + 1, DOWN)

            @pl.when(is_outer & (step == 4))
            def _():
                part_x(block_of(2, 1), 0).start()

            def folds(side):
                @pl.when(step - 1 - side >= 0)
                def _():
                    fold(step - 1 - side, side)

            each(2, folds)

        each(4, down_step)


        @pl.when(is_inner)
        def _():
            late_x(3, 0)

        def drain(turns, pair_turns):
            for count, send in ((pair_turns, pair_send), (turns, mid_send)):
                if count:
                    sent(wgu.at[:, pl.ds(0, count), pl.ds(0, depth), near], send.at[0])
                    sent(wd.at[pl.ds(0, count), near], send.at[1])

        @pl.when(is_inner)
        def _():
            drain(4, 3)

        @pl.when(is_outer)
        def _():
            drain(0, 2)

        sent(wgu.at[:, :, pl.ds(0, depth), near], y_send.at[0])
        sent(wd.at[pl.ds(0, 4), near], y_send.at[1])
        sent(wgu.at[:, :, :, near], c_send.at[0])
        sent(wd.at[:, near], c_send.at[1])
        for index in range(3):
            sent(rows.at[0, pl.ds(0, n_tok)], tok_send.at[index])
        scale_copy().wait_send()

    dma = pltpu.SemaphoreType.DMA
    turns, parts = 4, DOWN + 1
    pl.run_scoped(
        phases,
        dma((DOWN + 6,)), dma, dma, dma((2,)), dma((2,)), dma((turns - 1, parts)), dma((turns - 1, parts)),
        dma((2,)), dma((turns, parts)), dma((2,)), dma((turns, 2, 2)), dma((3,)), dma((2 * PIECES + 1,)),
        dma((4,)),
    )
    fold(3, 1)

    def finish(index):
        block = block_of(outer * (index // 2) + inner * (3 - index // 2), index % 2)
        part_x(block, 0).wait_recv()
        part_z(block).wait_recv()
        total = staged[block, 0, 0].astype(jnp.float32) + landed_x[block, 0].astype(jnp.float32)
        total = total + landed_z[block].astype(jnp.float32)
        result[:, pl.ds(pl.multiple_of(block * cols, cols), cols)] = total.astype(result.dtype)
        out_copy(block).start()

    each(8, finish)

    sent(landed_z, pz_send)

    @pl.when(is_inner)
    def _():
        sent(staged.at[pl.ds(0, 4)], px_send)

    @pl.when(is_outer)
    def _():
        sent(staged.at[pl.ds(0, 3)], px_send)
        sent(staged.at[0], pf_send)

    pltpu.make_async_copy(result, out_ref, out_sem).wait()


def kernel_body(tokens, norm_gain, gate_weight, gate_scale, up_weight, up_scale, down_weight, down_scale, sizes):
    n_fs = sizes[1]
    n_tok, width = tokens.shape
    depth = gate_weight.shape[0]
    all_units = gate_weight.shape[1]
    units = all_units // (2 * sizes[0])
    cols = down_weight.shape[1]
    anywhere = pl.BlockSpec(memory_space=pl.ANY)
    bf, wide = jnp.bfloat16, jnp.float32
    dma = pltpu.SemaphoreType.DMA
    turns = 4
    return pl.pallas_call(
        ffn_kernel,
        out_shape=jax.ShapeDtypeStruct((n_tok, width), bf),
        in_specs=[anywhere] * 8,
        out_specs=anywhere,
        scratch_shapes=[
            pltpu.VMEM((n_tok, width), bf),
            pltpu.VMEM((1, width), wide),
            pltpu.VMEM((all_units // 128, 128), wide),
            pltpu.VMEM((all_units // 128, 128), wide),
            pltpu.VMEM((1, width), wide),
            pltpu.VMEM((2, depth, 2 * units), wide),
            pltpu.VMEM((2 * units, cols), wide),
            pltpu.VMEM((2, n_fs // 2, 2 * depth, 2 * units), bf),
            pltpu.VMEM((n_fs, 2 * units, cols), bf),
            pltpu.VMEM((2, turns, depth, units), bf),
            pltpu.VMEM((turns, units, cols), bf),
            pltpu.VMEM((2, 2, units), wide),
            pltpu.VMEM((2, 2 * n_tok, width), bf),
            pltpu.VMEM((2, 2, 2 * n_tok, 2 * units), wide),
            pltpu.VMEM((2, 2 * n_tok, 2 * units), bf),
            pltpu.VMEM((n_fs, 2, 2, n_tok, cols), bf),
            pltpu.VMEM((n_fs, 2, n_tok, cols), bf),
            pltpu.VMEM((n_fs, n_tok, cols), bf),
            pltpu.VMEM((n_fs, n_tok, cols), bf),
            pltpu.VMEM((4, n_tok, cols), bf),
            pltpu.VMEM((n_tok, width), bf),
            dma, dma, dma((n_fs, 2)), dma, dma((n_fs,)), dma,
        ],
        compiler_params=pltpu.CompilerParams(
            collective_id=0, has_side_effects=True, vmem_limit_bytes=62 * 1024 * 1024
        ),
    )(
        tokens, norm_gain[None, :], gate_weight, gate_scale.reshape(-1, 128), up_weight, up_scale.reshape(-1, 128),
        down_weight, down_scale[None, :],
    )


def fits_kernel(mesh, tokens, gate_weight, down_weight):
    n_rep, n_fs, n_tp = (mesh.shape[name] for name in ("rep", "fs", "tp"))
    units = gate_weight.shape[1] // (n_tp * n_rep * 2)
    aligned = units % 128 == 0 and down_weight.shape[1] // n_fs % 128 == 0
    aligned = aligned and gate_weight.shape[0] // n_fs % (32 * CUTS) == 0
    return aligned and n_rep == 2 and n_fs == 8 and n_tp == 2


def solution(mesh):
    sizes = tuple(mesh.shape[name] for name in ("rep", "fs", "tp"))

    def run(tokens, norm_gain, gate_weight, gate_scale, up_weight, up_scale, down_weight, down_scale):
        chosen = body
        if fits_kernel(mesh, tokens, gate_weight, down_weight):
            chosen = functools.partial(kernel_body, sizes=sizes)
        return jax.shard_map(
            chosen,
            mesh=mesh,
            in_specs=(
                P(("rep", "fs", "tp"), None),
                P(),
                P("fs", "tp"),
                P("tp"),
                P("fs", "tp"),
                P("tp"),
                P("tp", "fs"),
                P(),
            ),
            out_specs=P(("rep", "fs", "tp"), None),
            check_vma=False,
        )(tokens, norm_gain, gate_weight, gate_scale, up_weight, up_scale, down_weight, down_scale)

    return run
```

```python
import functools

import jax
import jax.numpy as jnp
from jax import lax
from jax.experimental import pallas as pl
from jax.experimental.pallas import tpu as pltpu
from jax.sharding import PartitionSpec as P

EPS_VALUE = 1e-06


def from_partner(shard, axis, distance):
    return lax.ppermute(shard, axis, [(i, i ^ 1 << distance) for i in range(lax.axis_size(axis))])


def normalize(token_rows, norm_gain):
    values = token_rows.astype(jnp.float32)
    inverse = lax.rsqrt(jnp.mean(values * values, axis=-1, keepdims=True) + EPS_VALUE)
    return (values * inverse * norm_gain).astype(jnp.bfloat16)


def body(tokens, norm_gain, gate_weight, gate_scale, up_weight, up_scale, down_weight, down_scale):
    normed = normalize(tokens, norm_gain)
    gate_bf = gate_weight.astype(jnp.bfloat16)
    up_bf = up_weight.astype(jnp.bfloat16)
    down_bf = down_weight.astype(jnp.bfloat16)
    rep_index = lax.axis_index("rep")
    half_cols = gate_bf.shape[1] // 2
    half_rows = down_bf.shape[0] // 2
    own_gate = lax.dynamic_slice_in_dim(gate_bf, rep_index * half_cols, half_cols, 1)
    own_up = lax.dynamic_slice_in_dim(up_bf, rep_index * half_cols, half_cols, 1)
    own_down = lax.dynamic_slice_in_dim(down_bf, rep_index * half_rows, half_rows, 0)
    own_parts = (
        lax.all_gather(own_gate, "fs", axis=0, tiled=True),
        lax.all_gather(own_up, "fs", axis=0, tiled=True),
        lax.all_gather(own_down, "fs", axis=1, tiled=True),
    )
    far_parts = from_partner((own_parts[0], own_parts[1], own_parts[2]), "rep", 0)
    is_first = rep_index == 0

    def joined(own_part, far_part, axis_dim):
        return jnp.where(
            is_first,
            jnp.concatenate([own_part, far_part], axis_dim),
            jnp.concatenate([far_part, own_part], axis_dim),
        )

    gate_full = joined(own_parts[0], far_parts[0], 1)
    up_full = joined(own_parts[1], far_parts[1], 1)
    down_full = joined(own_parts[2], far_parts[2], 0)
    slab_rows = lax.all_gather(normed, "tp", axis=0, tiled=True)
    gate_pre = jnp.dot(slab_rows, gate_full, preferred_element_type=jnp.float32) * gate_scale
    up_pre = jnp.dot(slab_rows, up_full, preferred_element_type=jnp.float32) * up_scale
    hidden = (jax.nn.silu(gate_pre) * up_pre).astype(jnp.bfloat16)
    partial_value = (
        jnp.dot(hidden, down_full, preferred_element_type=jnp.float32) * down_scale
    ).astype(jnp.bfloat16)
    partial_value = lax.optimization_barrier(partial_value)
    return lax.psum_scatter(
        partial_value.astype(jnp.float32).astype(jnp.bfloat16),
        "tp",
        scatter_dimension=0,
        tiled=True,
    )


MESH = pl.DeviceIdType.MESH
CUTS = 8
DOWN = 2 * CUTS
QUARTER = DOWN // 4
PIECES = 4


def each(count, step):
    def go(index, carry):
        step(index)
        return carry

    lax.fori_loop(0, count, go, 0)


def ffn_kernel(
    tok_ref, gain_ref, gate_ref, gscale_ref, up_ref, uscale_ref, down_ref, dscale_ref, out_ref,
    tok, gain, gscale, uscale, dscale, raw_gu, raw_d, wgu, wd, tgu, td, scales, rows, acc, hid,
    staged, landed_x, summed, landed_z, landed_f, result,
    out_sem, px_send, px_recv, pz_send, pz_recv, pf_send,
):
    n_tok = tok.shape[0]
    piece_tok = n_tok // PIECES
    units = tgu.shape[3]
    depth = tgu.shape[2]
    fine = depth // CUTS
    cols = wd.shape[2]

    rep = lax.axis_index("rep")
    fs = lax.axis_index("fs")
    tp = lax.axis_index("tp")
    z = fs // 2
    y = fs % 2
    side_z = z // 2
    inner = (z + side_z) % 2
    outer = 1 - inner
    is_inner = inner == 1
    is_outer = inner == 0
    z_pair = 1 + 4 * side_z - z

    pair_dev = (rep, z_pair * 2 + y, tp)
    mid_dev = (rep, (3 - z) * 2 + y, tp)
    y_dev = (rep, z * 2 + 1 - y, tp)
    x_dev = (1 - rep, fs, tp)
    c_dev = (rep, fs, 1 - tp)

    def remote(src, dst, send, recv, device):
        return pltpu.make_async_remote_copy(
            src_ref=src, dst_ref=dst, send_sem=send, recv_sem=recv, device_id=device, device_id_type=MESH
        )

    def shard_z(turn):
        if isinstance(turn, int):
            return (z, z_pair, 2 - side_z, 3 - 3 * side_z)[turn]
        late = turn // 2
        odd = turn % 2
        early = (1 - odd) * z + odd * z_pair
        return (1 - late) * early + late * ((1 - odd) * (2 - side_z) + odd * (3 - 3 * side_z))

    def part_x(block, far):
        return remote(
            staged.at[block, far, 1], landed_x.at[block, far], px_send, px_recv.at[block, far], x_dev
        )

    def part_z(block):
        return remote(summed.at[block], landed_z.at[block], pz_send, pz_recv.at[block], pair_dev)

    def block_of(turn, side):
        return shard_z(turn) * 2 + y + side - 2 * side * y

    def z_first(turn, side):
        return ((turn < 2) & ((side == 1) | (turn + inner == 1))) | ((turn == 3) & (side == 0))

    def fold(turn, side):
        block = block_of(turn, side)

        @pl.when(is_inner | jnp.logical_not(z_first(turn, side)))
        def _():
            part_x(block, 1).wait_recv()
            total = staged[block, 1, 0].astype(jnp.float32) + landed_x[block, 1].astype(jnp.float32)
            summed[block] = total.astype(jnp.bfloat16)
            part_z(block).start()

    def out_copy(block):
        span = pl.ds(pl.multiple_of(block * cols, cols), cols)
        return pltpu.make_async_copy(result.at[:, span], out_ref.at[:, span], out_sem)

    def sent(src, send):
        remote(src, src, send, px_recv.at[0, 0], c_dev).wait_send()

    near = pl.ds(0, units)

    def phases(
        load_sem, scale_send, scale_recv, pair_send, mid_send, main_recv, thru_recv, y_send, y_recv, c_send, c_recv,
        tok_send, tok_recv, pf_recv,
    ):
        barrier = pltpu.get_barrier_semaphore()
        for device in (pair_dev, y_dev, x_dev, c_dev):
            pl.semaphore_signal(barrier, inc=1, device_id=device, device_id_type=MESH)

        @pl.when(is_inner)
        def _():
            pl.semaphore_signal(barrier, inc=1, device_id=mid_dev, device_id_type=MESH)

        def main_at(shard, shard_y, part, core):
            lanes = pl.ds(pl.multiple_of(core * units, 128), units)
            if isinstance(part, int) and part == DOWN:
                return wd.at[shard * 2 + shard_y, lanes]
            start = pl.multiple_of(shard_y * depth + (part % CUTS) * fine, fine)
            return wgu.at[part // CUTS, shard, pl.ds(start, fine), lanes]

        def thru_at(turn, part):
            if isinstance(part, int) and part == DOWN:
                return td.at[turn]
            start = pl.multiple_of((part % CUTS) * fine, fine)
            return tgu.at[part // CUTS, turn, pl.ds(start, fine)]

        def kind_of(part):
            return 1 if isinstance(part, int) and part == DOWN else 0

        def pair_copy(kind, part):
            send = pair_send.at[kind_of(part)]
            if kind == 0:
                return remote(thru_at(0, part), main_at(z, y, part, tp), send, main_recv.at[0, part], pair_dev)
            if kind == 1:
                return remote(main_at(z, y, part, tp), thru_at(1, part), send, thru_recv.at[0, part], pair_dev)
            return remote(
                thru_at(kind, part), main_at(shard_z(kind), y, part, tp), send, main_recv.at[kind - 1, part], pair_dev
            )

        def mid_copy(kind, part):
            send = mid_send.at[kind_of(part)]
            turn = 2 + kind // 2
            if kind % 2 == 0:
                ref = main_at(shard_z(kind // 2), y, part, tp)
                return remote(ref, ref, send, main_recv.at[turn - 1, part], mid_dev)
            return remote(thru_at(kind // 2, part), thru_at(turn, part), send, thru_recv.at[turn - 1, part], mid_dev)

        def main_in(turn, part):
            ref = main_at(shard_z(turn), y, part, tp)
            return remote(ref, ref, pair_send.at[0], main_recv.at[turn - 1, part], pair_dev)

        def thru_in(turn, part):
            ref = thru_at(turn, part)
            return remote(ref, ref, pair_send.at[0], thru_recv.at[turn - 1, part], pair_dev)

        def y_copy(turn, part):
            ref = main_at(shard_z(turn), y, part, tp)
            return remote(ref, ref, y_send.at[kind_of(part)], y_recv.at[turn, part], y_dev)

        def y_in(turn, part):
            ref = main_at(shard_z(turn), 1 - y, part, tp)
            return remote(ref, ref, y_send.at[kind_of(part)], y_recv.at[turn, part], y_dev)

        def c_copy(turn, side, part):
            ref = main_at(shard_z(turn), y + side - 2 * side * y, part, tp)
            return remote(ref, ref, c_send.at[kind_of(part)], c_recv.at[turn, side, kind_of(part)], c_dev)

        def c_in(turn, side, part):
            shard_y = y + side - 2 * side * y
            if part == DOWN:
                ref = main_at(shard_z(turn), shard_y, DOWN, 1 - tp)
            else:
                spare = pl.ds(pl.multiple_of((1 - tp) * units, 128), units)
                start = pl.multiple_of(shard_y * depth, depth)
                ref = wgu.at[:, shard_z(turn), pl.ds(start, depth), spare]
            return remote(ref, ref, c_send.at[kind_of(part)], c_recv.at[turn, side, kind_of(part)], c_dev)

        def tok_pair(piece):
            part = pl.ds(piece * piece_tok, piece_tok)
            return remote(
                rows.at[0, part], rows.at[1, part], tok_send.at[0], tok_recv.at[piece], pair_dev
            )

        def tok_far(piece):
            return remote(
                rows.at[1, pl.ds(piece * piece_tok, piece_tok)],
                rows.at[1, pl.ds(n_tok + piece * piece_tok, piece_tok)],
                tok_send.at[1], tok_recv.at[PIECES + piece], x_dev,
            )

        def tok_x():
            return remote(
                rows.at[0, pl.ds(0, n_tok)], rows.at[0, pl.ds(n_tok, n_tok)],
                tok_send.at[2], tok_recv.at[2 * PIECES], x_dev,
            )

        def early_z(block):
            return remote(staged.at[block, 1, 0], landed_z.at[block], pz_send, pz_recv.at[block], pair_dev)

        def place_of(turn, side):
            return side * (shard_z(turn) - 2 * side_z) + (1 - side) * (2 + turn // 2)

        def early_far(block, place):
            return remote(
                staged.at[block, 1, 1], landed_f.at[place], pf_send, pf_recv.at[place], pair_dev
            )

        def scale_copy():
            return remote(scales.at[tp], scales.at[tp], scale_send, scale_recv, c_dev)

        def scale_in():
            return remote(scales.at[1 - tp], scales.at[1 - tp], scale_send, scale_recv, c_dev)

        base = rep * 2 * units
        both = pl.ds(pl.multiple_of(base, 128), 2 * units)
        loads = []
        for part in range(DOWN):
            source = gate_ref if part // CUTS == 0 else up_ref
            span = pl.ds((part % CUTS) * fine, fine)
            loads.append((source.at[span, both], raw_gu.at[part // CUTS, span]))
        loads.append((down_ref.at[both], raw_d))
        loads += [(tok_ref, tok), (gain_ref, gain), (gscale_ref, gscale), (uscale_ref, uscale), (dscale_ref, dscale)]
        loads = [pltpu.make_async_copy(*pair, load_sem.at[index]) for index, pair in enumerate(loads)]
        for index in (0, 1, DOWN + 1, DOWN + 2, *range(2, DOWN + 1), DOWN + 3, DOWN + 4, DOWN + 5):
            loads[index].start()

        mine = pl.ds(pl.multiple_of(outer * units, 128), units)
        theirs = pl.ds(pl.multiple_of(inner * units, 128), units)
        lanes = pl.ds(pl.multiple_of(tp * units, 128), units)

        def round_part(part):
            loads[part].wait()
            span = slice((part % CUTS) * fine, (part % CUTS + 1) * fine)
            start = pl.multiple_of(y * depth + (part % CUTS) * fine, fine)
            wgu[part // CUTS, z, pl.ds(start, fine), lanes] = raw_gu[part // CUTS, span, mine].astype(jnp.bfloat16)
            tgu[part // CUTS, 0, span] = raw_gu[part // CUTS, span, theirs].astype(jnp.bfloat16)

        def send_part(part):
            pair_copy(0, part).start()
            y_copy(0, part).start()

            @pl.when(is_inner)
            def _():
                mid_copy(0, part).start()

            c_copy(0, 0, part).start()

        round_part(0)
        pl.semaphore_wait(barrier, 4 + inner)
        send_part(0)
        round_part(1)
        send_part(1)
        loads[DOWN + 1].wait()
        loads[DOWN + 2].wait()
        values = tok[...].astype(jnp.float32)
        inverse = lax.rsqrt(jnp.mean(values * values, axis=-1, keepdims=True) + EPS_VALUE)
        rows[0, :n_tok] = (values * inverse * gain[...]).astype(jnp.bfloat16)
        tok_x().start()
        for part in range(2, DOWN):
            round_part(part)
            send_part(part)
        for piece in range(PIECES):
            tok_pair(piece).start()

        @pl.when(is_inner)
        def _():
            each(DOWN, lambda part: mid_copy(1, part).start())

        @pl.when(is_outer)
        def _():
            each(DOWN, lambda part: pair_copy(1, part).start())

        for index in (DOWN + 3, DOWN + 4, DOWN + 5):
            loads[index].wait()
        first_row = (base + outer * units) // 128
        for index in range(units // 128):
            span = slice(index * 128, (index + 1) * 128)
            scales[tp, 0:1, span] = gscale[pl.ds(first_row + index, 1), :]
            scales[tp, 1:2, span] = uscale[pl.ds(first_row + index, 1), :]
        scale_copy().start()
        loads[DOWN].wait()
        wd[fs, lanes] = raw_d[mine].astype(jnp.bfloat16)
        td[0] = raw_d[theirs].astype(jnp.bfloat16)
        c_copy(0, 0, DOWN).start()

        @pl.when(is_outer)
        def _():
            pair_copy(0, DOWN).start()
            pair_copy(1, DOWN).start()

        def take_main(turn, part):
            main_in(turn, part).wait_recv()
            y_copy(turn, part).start()
            c_copy(turn, 0, part).start()

        def take_y(turn, part):
            y_in(turn, part).wait_recv()
            c_copy(turn, 1, part).start()

        def take_rows(piece):
            tok_pair(piece).wait_recv()
            tok_far(piece).start()

        def c_wait(turn):
            for side in range(2):
                c_in(turn, side, 0).wait_recv()

        def term(far, matrix, turn):
            shard = shard_z(turn)
            span = pl.ds(pl.multiple_of(shard * 2 * depth, 2 * depth), 2 * depth)
            return jnp.dot(rows[far, :, span], wgu[matrix, shard], preferred_element_type=jnp.float32)

        def add_early(part):
            far, matrix = part // 2, part % 2

            @pl.when(part == 2)
            def _():
                for piece in range(PIECES):
                    tok_far(piece).wait_recv()

            acc[matrix, far] = term(far, matrix, 0)
            acc[matrix, far] += term(far, matrix, 1)

        def add_late(part):
            acc[part % 2, part // 2] += term(part // 2, part % 2, 2)

        def half_term(far, matrix, span, side):
            shard = shard_z(3)
            shard_y = y + side - 2 * side * y
            start = pl.multiple_of((shard * 2 + shard_y) * depth, depth)
            inside = pl.multiple_of(shard_y * depth, depth)
            return jnp.dot(
                rows[far, span, pl.ds(start, depth)], wgu[matrix, shard, pl.ds(inside, depth)],
                preferred_element_type=jnp.float32,
            )

        def add_last(part):
            acc[part % 2, part // 2] += half_term(part // 2, part % 2, pl.ds(0, 2 * n_tok), 0)

        def first(part):
            take_main(1, part)

            @pl.when(is_inner)
            def _():
                mid_copy(2, part).start()

            take_y(0, part)

        each(DOWN, first)

        @pl.when(is_inner)
        def _():
            each(DOWN, lambda part: take_main(2, part))

        @pl.when(is_outer)
        def _():
            y_copy(0, DOWN).start()

        def second(part):
            @pl.when(is_inner)
            def _():
                thru_in(2, part).wait_recv()
                pair_copy(2, part).start()

            take_y(1, part)

            for piece in range(2):
                @pl.when(part == QUARTER * (piece + 2) - 1)
                def _():
                    take_rows(piece)

        each(DOWN, second)
        take_rows(2)

        def pass_outward(part):
            thru_in(1, part).wait_recv()
            mid_copy(3, part).start()

        @pl.when(is_inner)
        def _():
            def third(part):
                take_main(3, part)
                take_y(2, part)

                @pl.when(part == 2 * QUARTER - 1)
                def _():
                    take_rows(3)

                @pl.when(part >= 3 * QUARTER)
                def _():
                    pass_outward(part - 3 * QUARTER)

            each(DOWN, third)
            y_copy(0, DOWN).start()

        @pl.when(is_outer)
        def _():
            take_rows(3)

        tok_x().wait_recv()
        c_wait(0)
        c_wait(1)

        @pl.when(is_inner)
        def _():
            c_wait(2)
            c_in(3, 0, 0).wait_recv()

            def fourth(chunk):
                @pl.when(chunk < 3)
                def _():
                    for ahead in range(QUARTER):
                        pass_outward(QUARTER * (chunk + 1) + ahead)

                @pl.when(chunk == 2)
                def _():
                    mid_copy(1, DOWN).start()
                    mid_copy(0, DOWN).start()

                add_early(chunk)
                add_late(chunk)
                for part in [QUARTER * chunk + index for index in range(QUARTER)]:
                    thru_in(3, part).wait_recv()
                    pair_copy(3, part).start()
                    take_y(3, part)
                add_last(chunk)

            each(4, fourth)
            pair_copy(0, DOWN).start()

        @pl.when(is_outer)
        def _():
            def fourth(chunk):
                for part in [QUARTER * chunk + index for index in range(QUARTER)]:
                    take_main(2, part)

                    @pl.when(chunk > 0)
                    def _():
                        take_y(2, part - QUARTER)

                add_early(chunk)

            each(4, fourth)

            def fifth(chunk):
                for part in [QUARTER * chunk + index for index in range(QUARTER)]:
                    take_main(3, part)

                    @pl.when(chunk == 0)
                    def _():
                        take_y(2, part + DOWN - QUARTER)

                    @pl.when(chunk > 0)
                    def _():
                        take_y(3, part - QUARTER)

                @pl.when(chunk == 0)
                def _():
                    take_y(0, DOWN)
                    c_wait(2)

                add_late(chunk)

            each(4, fifth)
            c_in(3, 0, 0).wait_recv()
            for part in range(QUARTER // 2):
                take_y(3, DOWN - QUARTER + part)
            each(2, add_last)
            for part in range(QUARTER // 2, QUARTER):
                take_y(3, DOWN - QUARTER + part)
            each(2, lambda chunk: add_last(chunk + 2))
            c_in(0, 1, DOWN).wait_recv()

        def send_off(turn, side, far, near_x):
            block = block_of(turn, side)
            ahead = z_first(turn, side)
            crossing = far + inner == 1

            held = is_outer & (turn == 2) & (side == 1) & (far == 0)

            @pl.when((near_x == 1) & jnp.logical_not((ahead & crossing) | held))
            def _():
                part_x(block, far).start()

            @pl.when(ahead & crossing & is_outer)
            def _():
                @pl.when(near_x == 1)
                def _():
                    early_far(block, place_of(turn, side)).start()

                @pl.when(near_x == 0)
                def _():
                    early_z(block).start()

        def scale_of(block):
            return dscale[:, pl.ds(pl.multiple_of(block * cols, cols), cols)]

        scale_in().wait_recv()
        c_in(3, 1, 0).wait_recv()
        c_in(0, 0, DOWN).wait_recv()

        def activate(index):
            far = 1 - index % 2
            near_x = 1 - index // 2
            span = pl.ds(pl.multiple_of(near_x * n_tok, n_tok), n_tok)
            pre = []

            @pl.when(index == 1)
            def _():
                take_main(1, DOWN)

            for matrix in range(2):
                last = half_term(far, matrix, span, 1)
                scale = jnp.concatenate(
                    [scales[0, matrix:matrix + 1], scales[1, matrix:matrix + 1]], axis=1
                )
                pre.append((acc[matrix, far, span] + last) * scale)
            hid[far, span] = (jax.nn.silu(pre[0]) * pre[1]).astype(jnp.bfloat16)

            def one(side, carry):
                block = block_of(0, side)
                product = jnp.dot(hid[far, span], wd[block], preferred_element_type=jnp.float32) * scale_of(block)
                staged[block, far, near_x] = product.astype(jnp.bfloat16)
                send_off(0, side, far, near_x)
                return carry

            lax.fori_loop(0, 1 + outer, one, 0)

        each(4, activate)

        def produce(turn, side):
            block = block_of(turn, side)

            def tile(index):
                far = 1 - index
                product = jnp.dot(hid[far], wd[block], preferred_element_type=jnp.float32) * scale_of(block)
                staged[block, far] = product.astype(jnp.bfloat16).reshape(2, n_tok, cols)
                for near_x in (1, 0):
                    send_off(turn, side, far, near_x)

            each(2, tile)

        def late_x(turn, side):
            block = block_of(turn, side)
            place = place_of(turn, side)
            early_far(block, place).wait_recv()
            total = staged[block, 0, 1].astype(jnp.float32) + landed_f[place].astype(jnp.float32)
            staged[block, 0, 1] = total.astype(jnp.bfloat16)
            part_x(block, 0).start()

        def down_step(index):
            step = index + 1
            swap = inner * (step // 3) * (1 - step // 4)

            @pl.when(is_inner & (step == 2))
            def _():
                take_main(2, DOWN)

            @pl.when(is_inner & (step == 4))
            def _():
                late_x(0, 0)

            @pl.when(step > 1)
            def _():
                take_y(step - 1, DOWN)

            def sides(order):
                side = order + swap - 2 * order * swap
                turn = step - side

                @pl.when((turn < 4) & ((side == 0) | (turn > 0) | is_inner))
                def _():
                    @pl.when(is_inner & (side == 0) & (turn == 3))
                    def _():
                        late_x(1, 1)
                        take_main(3, DOWN)

                    @pl.when(is_inner & (step == 1) & (side == 1))
                    def _():
                        take_y(0, DOWN)

                    c_in(turn, side, DOWN).wait_recv()
                    produce(turn, side)

            each(2, sides)

            @pl.when(is_inner)
            def _():
                @pl.when(step == 1)
                def _():
                    thru_in(2, DOWN).wait_recv()
                    pair_copy(2, DOWN).start()
                    thru_in(1, DOWN).wait_recv()
                    mid_copy(3, DOWN).start()
                    mid_copy(2, DOWN).start()

                @pl.when(step == 2)
                def _():
                    thru_in(3, DOWN).wait_recv()
                    pair_copy(3, DOWN).start()

                @pl.when(step == 4)
                def _():
                    late_x(0, 1)

            @pl.when(is_outer & (step < 3))
            def _():
                take_main(step + 1, DOWN)

            @pl.when(is_outer & (step == 4))
            def _():
                part_x(block_of(2, 1), 0).start()

            def folds(side):
                @pl.when(step - 1 - side >= 0)
                def _():
                    fold(step - 1 - side, side)

            each(2, folds)

        each(4, down_step)


        @pl.when(is_inner)
        def _():
            late_x(3, 0)

        def drain(turns, pair_turns):
            for count, send in ((pair_turns, pair_send), (turns, mid_send)):
                if count:
                    sent(wgu.at[:, pl.ds(0, count), pl.ds(0, depth), near], send.at[0])
                    sent(wd.at[pl.ds(0, count), near], send.at[1])

        @pl.when(is_inner)
        def _():
            drain(4, 3)

        @pl.when(is_outer)
        def _():
            drain(0, 2)

        sent(wgu.at[:, :, pl.ds(0, depth), near], y_send.at[0])
        sent(wd.at[pl.ds(0, 4), near], y_send.at[1])
        sent(wgu.at[:, :, :, near], c_send.at[0])
        sent(wd.at[:, near], c_send.at[1])
        for index in range(3):
            sent(rows.at[0, pl.ds(0, n_tok)], tok_send.at[index])
        scale_copy().wait_send()

    dma = pltpu.SemaphoreType.DMA
    turns, parts = 4, DOWN + 1
    pl.run_scoped(
        phases,
        dma((DOWN + 6,)), dma, dma, dma((2,)), dma((2,)), dma((turns - 1, parts)), dma((turns - 1, parts)),
        dma((2,)), dma((turns, parts)), dma((2,)), dma((turns, 2, 2)), dma((3,)), dma((2 * PIECES + 1,)),
        dma((4,)),
    )
    fold(3, 1)

    def finish(index):
        block = block_of(outer * (index // 2) + inner * (3 - index // 2), index % 2)
        part_x(block, 0).wait_recv()
        part_z(block).wait_recv()
        total = staged[block, 0, 0].astype(jnp.float32) + landed_x[block, 0].astype(jnp.float32)
        total = total + landed_z[block].astype(jnp.float32)
        result[:, pl.ds(pl.multiple_of(block * cols, cols), cols)] = total.astype(result.dtype)
        out_copy(block).start()

    each(8, finish)

    sent(landed_z, pz_send)

    @pl.when(is_inner)
    def _():
        sent(staged.at[pl.ds(0, 4)], px_send)

    @pl.when(is_outer)
    def _():
        sent(staged.at[pl.ds(0, 3)], px_send)
        sent(staged.at[0], pf_send)

    pltpu.make_async_copy(result, out_ref, out_sem).wait()


def kernel_body(tokens, norm_gain, gate_weight, gate_scale, up_weight, up_scale, down_weight, down_scale, sizes):
    n_fs = sizes[1]
    n_tok, width = tokens.shape
    depth = gate_weight.shape[0]
    all_units = gate_weight.shape[1]
    units = all_units // (2 * sizes[0])
    cols = down_weight.shape[1]
    anywhere = pl.BlockSpec(memory_space=pl.ANY)
    bf, wide = jnp.bfloat16, jnp.float32
    dma = pltpu.SemaphoreType.DMA
    turns = 4
    return pl.pallas_call(
        ffn_kernel,
        out_shape=jax.ShapeDtypeStruct((n_tok, width), bf),
        in_specs=[anywhere] * 8,
        out_specs=anywhere,
        scratch_shapes=[
            pltpu.VMEM((n_tok, width), bf),
            pltpu.VMEM((1, width), wide),
            pltpu.VMEM((all_units // 128, 128), wide),
            pltpu.VMEM((all_units // 128, 128), wide),
            pltpu.VMEM((1, width), wide),
            pltpu.VMEM((2, depth, 2 * units), wide),
            pltpu.VMEM((2 * units, cols), wide),
            pltpu.VMEM((2, n_fs // 2, 2 * depth, 2 * units), bf),
            pltpu.VMEM((n_fs, 2 * units, cols), bf),
            pltpu.VMEM((2, turns, depth, units), bf),
            pltpu.VMEM((turns, units, cols), bf),
            pltpu.VMEM((2, 2, units), wide),
            pltpu.VMEM((2, 2 * n_tok, width), bf),
            pltpu.VMEM((2, 2, 2 * n_tok, 2 * units), wide),
            pltpu.VMEM((2, 2 * n_tok, 2 * units), bf),
            pltpu.VMEM((n_fs, 2, 2, n_tok, cols), bf),
            pltpu.VMEM((n_fs, 2, n_tok, cols), bf),
            pltpu.VMEM((n_fs, n_tok, cols), bf),
            pltpu.VMEM((n_fs, n_tok, cols), bf),
            pltpu.VMEM((4, n_tok, cols), bf),
            pltpu.VMEM((n_tok, width), bf),
            dma, dma, dma((n_fs, 2)), dma, dma((n_fs,)), dma,
        ],
        compiler_params=pltpu.CompilerParams(
            collective_id=0, has_side_effects=True, vmem_limit_bytes=62 * 1024 * 1024
        ),
    )(
        tokens, norm_gain[None, :], gate_weight, gate_scale.reshape(-1, 128), up_weight, up_scale.reshape(-1, 128),
        down_weight, down_scale[None, :],
    )


def fits_kernel(mesh, tokens, gate_weight, down_weight):
    n_rep, n_fs, n_tp = (mesh.shape[name] for name in ("rep", "fs", "tp"))
    units = gate_weight.shape[1] // (n_tp * n_rep * 2)
    aligned = units % 128 == 0 and down_weight.shape[1] // n_fs % 128 == 0
    aligned = aligned and gate_weight.shape[0] // n_fs % (32 * CUTS) == 0
    return aligned and n_rep == 2 and n_fs == 8 and n_tp == 2


def solution(mesh):
    sizes = tuple(mesh.shape[name] for name in ("rep", "fs", "tp"))

    def run(tokens, norm_gain, gate_weight, gate_scale, up_weight, up_scale, down_weight, down_scale):
        chosen = body
        if fits_kernel(mesh, tokens, gate_weight, down_weight):
            chosen = functools.partial(kernel_body, sizes=sizes)
        return jax.shard_map(
            chosen,
            mesh=mesh,
            in_specs=(
                P(("rep", "fs", "tp"), None),
                P(),
                P("fs", "tp"),
                P("tp"),
                P("fs", "tp"),
                P("tp"),
                P("tp", "fs"),
                P(),
            ),
            out_specs=P(("rep", "fs", "tp"), None),
            check_vma=False,
        )(tokens, norm_gain, gate_weight, gate_scale, up_weight, up_scale, down_weight, down_scale)

    return run
```
